256 devices in a mesh: sp: 16 (over y, x), tp: 16 (over z, core).
Axes of the slice: x: 4, y: 4, z: 8, core: 2. Of those that a mesh axis runs over, the one named last changes fastest.
Arguments:
- receptance: bfloat16 [4096, 1024], P('sp', 'tp'), may hold values from -6 to 6
- key_matrix: bfloat16 [4096, 1024], P('sp', 'tp'), may hold values from -6 to 6
- value_matrix: bfloat16 [4096, 1024], P('sp', 'tp'), may hold values from -6 to 6
- decay_input_term: bfloat16 [4096, 1024], P('sp', 'tp'), may hold values from -5 to 5
- decay_channel_offset: float32 [1024], P('tp'), may hold values from -12 to -2
- head_log_decay: float32 [4096, 16], P('sp', 'tp'), may hold values from -2 to 0
- context_step_logits: bfloat16 [4096, 1024], P('sp', 'tp'), may hold values from -16 to 4
- head_gate_rows: bfloat16 [4096, 1024], P('sp', 'tp'), may hold values from -6 to 6
- head_norm_scale: float32 [1024], P('tp'), may hold values from 0.1 to 1.9
- mixer_output_weight: bfloat16 [1024, 2048], replicated, may hold values from -0.1875 to 0.1875
- residual: bfloat16 [4096, 2048], P(('sp', 'tp')), may hold values from -6 to 6
- expert_norm_scale: float32 [2048], replicated, may hold values from 0.1 to 1.9
- expert_index_table: int32 [4096, 2], P(('sp', 'tp')), may hold values from 0 to 15, all different within a row; in each aligned block of 16 rows (0 to 15, 16 to 31, ...) at most 4 rows name the same one
- expert_router_scores: float32 [4096, 2], P(('sp', 'tp')), may hold values from -6 to 6
- expert_gate_weight: bfloat16 [16, 2048, 7168], P('sp', None, 'tp'), may hold values from -0.125 to 0.125
- expert_up_weight: bfloat16 [16, 2048, 7168], P('sp', None, 'tp'), may hold values from -0.125 to 0.125
- expert_down_weight: bfloat16 [16, 7168, 2048], P('sp', 'tp'), may hold values from -0.0625 to 0.0625
Outputs:
- layer_out: bfloat16 [4096, 2048], P(('sp', 'tp'))
The draws below stay inside these ranges and needn't reach their ends.
Inputs may be any that keep to these rules, and one draw needn't show every extreme that they name: `expert_index_table`: each row names 2 different experts. In each aligned block of 16 rows no expert is named more than 4 times, a bound that some block reaches.
All inputs are finite; a program needn't handle non-finite values.
Results may differ from the reference program's by a relative error of at most 0.018.
Values may be sent and summed in bfloat16 or wider, within the bound.
A program may use at most 64 MiB of HBM per device.

```python
import math
import jax
import jax.numpy as jnp
import numpy as np
from jax import lax

D = 2048
HEADS = 16
HEAD_CHANNELS = 64
FF = 7168
TOPK = 2
WIDTH = 1024
TOKENS = 4096
EXPERTS = 16
ROWS = 16
CAP = 4
N_TP = 16


def head_kinds(key):
    order = jax.random.permutation(jax.random.fold_in(key, 101), HEADS)
    slow = order < HEADS // 2
    return jnp.repeat(slow, HEAD_CHANNELS)


def noise(key, array_shape):
    return jnp.clip(jax.random.normal(key, array_shape, jnp.float32), -4.0, 4.0)


def draw_decay_channel_offset(key, part):
    slow = head_kinds(key)
    fast_level = jnp.repeat(jax.random.uniform(jax.random.fold_in(key, 102), (HEADS,), jnp.float32, -3.5, -3.0), HEAD_CHANNELS)
    jitter = jax.random.uniform(jax.random.fold_in(key, 103), (WIDTH,), jnp.float32, -0.5, 0.5)
    slow_level = math.log(0.17 / TOKENS)
    return jnp.where(slow, slow_level, fast_level) + jitter


def draw_context_step_logits(key, part):
    slow = head_kinds(key)
    level = jnp.where(slow, math.log(0.5 * HEAD_CHANNELS / TOKENS), 0.0)
    shifted = noise(jax.random.fold_in(key, 104), (TOKENS, WIDTH)) + level[None, :]
    return shifted.astype(jnp.bfloat16)


def draw_decay_input_term(key, part):
    offset = jax.random.uniform(jax.random.fold_in(key, 105), (TOKENS // 128, 1, 1), jnp.float32, -1.0, 1.0)
    shifted = noise(jax.random.fold_in(key, 106), (TOKENS // 128, 128, WIDTH)) + offset
    return shifted.reshape(TOKENS, WIDTH).astype(jnp.bfloat16)


def draw_head_log_decay(key, part):
    where_at = jax.random.randint(jax.random.fold_in(key, 107), (2,), 0, TOKENS)
    strength = jax.random.uniform(jax.random.fold_in(key, 108), (2, HEADS), jnp.float32, math.log(0.5), math.log(0.8))
    position = jnp.arange(TOKENS, dtype=jnp.int32)
    marked = (position[:, None, None] == where_at[None, :, None]).astype(jnp.float32)
    return jnp.sum(marked * strength[None, :, :], axis=1)


def level_of(own_key, dims, shards, smallest, high):
    def one(axis_at, shards_of):
        steps = jax.random.uniform(jax.random.fold_in(jax.random.fold_in(own_key, 6), axis_at), (shards_of,), jnp.float32, smallest / len(shards), high / len(shards))
        return jnp.repeat(jnp.exp(steps), dims[axis_at] // shards_of).reshape((-1,) + (1,) * (len(dims) - axis_at - 1))

    factor_of = one(*shards[0])
    for cut in shards[1:]:
        factor_of = factor_of * one(*cut)
    return factor_of


def shared_out(own_key, own, number, rows, amount, top, reach, skew):
    sequence = jax.random.permutation(own_key, amount)
    heavy_load, usual = portions_of(amount, rows * top, reach, skew, True), portions_of(amount, rows * top, reach, skew, False)
    places = jnp.arange(amount)

    def named(lengths, turn):
        used = int((lengths > 0).sum())
        fixed = max(1, used // 4)
        moved = fixed + (places - fixed + turn * (used - fixed)) % max(1, amount - fixed)
        return jnp.zeros((amount,), jnp.int32).at[sequence[jnp.where(places < fixed, places, moved)]].set(jnp.asarray(lengths, jnp.int32))

    lengths = jnp.where(number % 4 == 0, named(heavy_load, number // 4), named(usual, number - number // 4 - 1))
    mixed = jax.random.permutation(jax.random.fold_in(own, 3), amount)
    source_of, taker = mixed[0:amount // 2 * 2:2], mixed[1:amount // 2 * 2:2]
    margin = jnp.minimum(lengths[source_of] - 1, reach - lengths[taker]) // 2
    margin = jnp.where((source_of == sequence[0]) | (taker == sequence[0]) | (lengths[taker] == 0), 0, jnp.maximum(margin, 0))
    moved = jax.random.randint(jax.random.fold_in(own, 4), (amount // 2,), 0, 1 << 20) % (margin + 1)
    lengths = lengths.at[source_of].add(-moved).at[taker].add(moved)
    items = jnp.searchsorted(jnp.cumsum(lengths), jnp.arange(rows * top), side="right").astype(jnp.int32)
    table = items.reshape(top, rows).T
    table = table[jax.random.permutation(jax.random.fold_in(own, 1), rows)]
    turn = jax.random.randint(jax.random.fold_in(own, 2), (rows, 1), 0, top)
    return jnp.take_along_axis(table, (jnp.arange(top)[None, :] + turn) % top, axis=1)


def portions_of(number_of, total, most, skew, full):
    weights = [(1 << 20) // math.isqrt(standing ** skew) + 1 for standing in range(1, number_of + 1)]
    largest = most if full else min(most, max(-(-total // number_of), total * weights[0] // sum(weights)))
    least = 1 if total - largest >= number_of - 1 else 0
    counts, rest = [largest] + [least] * (number_of - 1), total - largest - least * (number_of - 1)
    while rest > 0:
        candidates = [i for i in range(1, number_of) if counts[i] < largest] or [i for i in range(1, number_of) if counts[i] < most]
        whole, budget = sum([weights[i] for i in candidates]), rest
        for i in candidates:
            extra = min(most - counts[i], max(1, budget * weights[i] // whole), rest)
            counts[i] = counts[i] + extra
            rest = rest - extra
    return np.array(counts)


def normal_values(stream_key, extent, scale, limit, pieces=(), kind=jnp.bfloat16):
    drawn = jax.random.normal(stream_key, extent, jnp.float32) * scale
    if len(pieces) > 0:
        drawn = level_of(stream_key, extent, pieces, -0.22, 0.18) * drawn
    return jnp.clip(drawn, min=-limit, max=limit).astype(kind)


def setup_inputs(seed: int = 0) -> dict:
    keys = jax.random.split(jax.random.key(seed), 18)
    receptance = normal_values(keys[0], (TOKENS, WIDTH), 1.0, 6.0, ((0, 16), (1, 16)))
    key_matrix = normal_values(keys[1], (TOKENS, WIDTH), 1.0, 6.0, ((0, 16), (1, 16)))
    value_matrix = normal_values(keys[2], (TOKENS, WIDTH), 1.0, 6.0, ((0, 16), (1, 16)))
    decay_input_term = draw_decay_input_term(jax.random.fold_in(keys[17], 71), 0)
    decay_channel_offset = draw_decay_channel_offset(jax.random.fold_in(keys[17], 71), 0)
    head_log_decay = draw_head_log_decay(jax.random.fold_in(keys[17], 71), 0)
    context_step_logits = draw_context_step_logits(jax.random.fold_in(keys[17], 71), 0)
    head_gate_rows = normal_values(keys[7], (TOKENS, WIDTH), 1.0, 6.0, ((0, 16), (1, 16)))
    head_norm_scale = jnp.clip(1.0 + 0.18 * jax.random.normal(keys[8], (WIDTH,), jnp.float32), 0.1, 1.9)
    mixer_output_weight = normal_values(keys[9], (WIDTH, D), WIDTH ** -0.5, 0.1875)
    residual = normal_values(keys[10], (TOKENS, D), 1.0, 6.0, ((0, 256),))
    expert_norm_scale = jnp.clip(1.0 + 0.18 * jax.random.normal(keys[11], (D,), jnp.float32), 0.1, 1.9)
    expert_index_table_keys = jax.random.split(jax.random.fold_in(keys[12], 1), TOKENS // ROWS)
    expert_index_table_turns = jax.random.permutation(jax.random.fold_in(keys[12], 3), TOKENS // ROWS)
    expert_index_table = jax.vmap(lambda own, number: shared_out(jax.random.fold_in(keys[12], 2), own, number, ROWS, EXPERTS, TOPK, CAP, 1))(expert_index_table_keys, expert_index_table_turns).reshape((TOKENS, TOPK))
    expert_router_scores = normal_values(keys[13], (TOKENS, TOPK), 1.5, 6.0, ((0, 256),), jnp.float32)
    expert_gate_weight = normal_values(keys[14], (EXPERTS, D, FF), D ** -0.5, 0.125, ((0, 16), (2, 16)))
    expert_up_weight = normal_values(keys[15], (EXPERTS, D, FF), D ** -0.5, 0.125, ((0, 16), (2, 16)))
    expert_down_weight = normal_values(keys[16], (EXPERTS, FF, D), FF ** -0.5, 0.0625, ((0, 16), (1, 16)))
    return {"receptance": receptance, "key_matrix": key_matrix, "value_matrix": value_matrix, "decay_input_term": decay_input_term, "decay_channel_offset": decay_channel_offset, "head_log_decay": head_log_decay, "context_step_logits": context_step_logits, "head_gate_rows": head_gate_rows, "head_norm_scale": head_norm_scale, "mixer_output_weight": mixer_output_weight, "residual": residual, "expert_norm_scale": expert_norm_scale, "expert_index_table": expert_index_table, "expert_router_scores": expert_router_scores, "expert_gate_weight": expert_gate_weight, "expert_up_weight": expert_up_weight, "expert_down_weight": expert_down_weight}


decay_factor = 0.6065306597126334
group_eps = 0.00064
norm_eps = 1e-06
key_eps = 1e-06
highest = lax.Precision.HIGHEST

def per_head_input(receptance, key_matrix, value_matrix, decay_input_term, decay_channel_offset, head_log_decay, context_step_logits):
    head_split_shape = (receptance.shape[0], head_log_decay.shape[1], HEAD_CHANNELS)
    read_vec = receptance.astype(jnp.float32).reshape(head_split_shape)
    key_vec = key_matrix.astype(jnp.float32).reshape(head_split_shape)
    value_vec = value_matrix.astype(jnp.float32).reshape(head_split_shape)
    decay_logits = (decay_input_term.astype(jnp.float32) + decay_channel_offset[None, :]).reshape(head_split_shape)
    decay_vector = jnp.exp(-decay_factor * jax.nn.sigmoid(decay_logits) + head_log_decay[:, :, None])
    learn_vec = jax.nn.sigmoid(context_step_logits.astype(jnp.float32)).reshape(head_split_shape)
    unit_vec = key_vec * lax.rsqrt(lax.optimization_barrier(jnp.sum(key_vec * key_vec, axis=-1, keepdims=True)) + key_eps)
    return (read_vec, decay_vector, -unit_vec, unit_vec * learn_vec, key_vec * learn_vec, value_vec)

def finish(mixer_out, head_norm_scale, head_gate_rows):
    average = lax.optimization_barrier(jnp.mean(mixer_out, axis=-1, keepdims=True))
    centred = mixer_out - average
    spread = lax.optimization_barrier(jnp.mean(centred * centred, axis=-1, keepdims=True))
    normed = (centred * lax.rsqrt(spread + group_eps)).reshape(mixer_out.shape[0], -1)
    return (normed * head_norm_scale[None, :] * head_gate_rows.astype(jnp.float32)).astype(jnp.bfloat16)

def advance(state_mat, packed):
    read_vec, decay_vector, erase_vec, write_vec, keyed_vec, value_vec = packed
    recall = jnp.einsum('hvk,hk->hv', state_mat, erase_vec, precision=highest)
    state_mat = state_mat * decay_vector[:, None, :] + recall[:, :, None] * write_vec[:, None, :] + value_vec[:, :, None] * keyed_vec[:, None, :]
    return (state_mat, jnp.einsum('hvk,hk->hv', state_mat, read_vec, precision=highest))

def expert_outputs(normed, expert_index_table, expert_gate_weight, expert_up_weight, expert_down_weight):
    block_count = TOKENS // ROWS
    chosen = expert_index_table.reshape(block_count, ROWS * TOPK)
    matches = (chosen[:, :, None] == jnp.arange(EXPERTS, dtype=jnp.int32)[None, None, :]).astype(jnp.int32)
    slot_of = lax.optimization_barrier(jnp.sum(jnp.cumsum(matches, axis=1) * matches, axis=2)) - 1
    block_of = jnp.arange(block_count, dtype=jnp.int32)[:, None]
    placing = (chosen * (block_count * CAP) + block_of * CAP + slot_of).astype(jnp.int32)
    token_of = (block_of * ROWS + jnp.arange(ROWS * TOPK, dtype=jnp.int32)[None, :] // TOPK).astype(jnp.int32)
    routing = jnp.full((EXPERTS * block_count * CAP,), TOKENS, jnp.int32).at[placing.reshape(-1)].set(token_of.reshape(-1))
    padded = jnp.concatenate([normed, jnp.zeros((1, D), jnp.bfloat16)], axis=0)
    block_width = FF // N_TP

    def one_expert(packed):
        slot_index, gate_mat, up_mat, down_mat = packed
        picked = padded[slot_index]
        gate_act = jnp.dot(picked, gate_mat, preferred_element_type=jnp.float32)
        up_act = jnp.dot(picked, up_mat, preferred_element_type=jnp.float32)
        hidden = (jax.nn.silu(gate_act) * up_act).astype(jnp.bfloat16)
        partials = jnp.einsum('rjf,jfd->jrd', hidden.reshape(-1, N_TP, block_width).astype(jnp.float32), down_mat.reshape(N_TP, block_width, D).astype(jnp.float32))
        rounded = lax.optimization_barrier(partials.astype(jnp.bfloat16))
        return lax.optimization_barrier(jnp.sum(rounded.astype(jnp.float32), axis=0)).astype(jnp.bfloat16)
    results = lax.map(one_expert, (routing.reshape(EXPERTS, -1), expert_gate_weight, expert_up_weight, expert_down_weight))
    flat_out = results.reshape(-1, D)
    return flat_out[placing.reshape(-1)].reshape(TOKENS, TOPK, D)

def reference(receptance, key_matrix, value_matrix, decay_input_term, decay_channel_offset, head_log_decay, context_step_logits, head_gate_rows, head_norm_scale, mixer_output_weight, residual, expert_norm_scale, expert_index_table, expert_router_scores, expert_gate_weight, expert_up_weight, expert_down_weight):
    input_rows = per_head_input(receptance, key_matrix, value_matrix, decay_input_term, decay_channel_offset, head_log_decay, context_step_logits)
    state_zero = jnp.zeros((HEADS, HEAD_CHANNELS, HEAD_CHANNELS), jnp.float32)
    _, mixer_out = lax.scan(advance, state_zero, input_rows)
    attended = finish(mixer_out, head_norm_scale, head_gate_rows)
    mixed = (residual.astype(jnp.float32) + jnp.dot(attended, mixer_output_weight, preferred_element_type=jnp.float32)).astype(jnp.bfloat16)
    mixed_f = mixed.astype(jnp.float32)
    normed = (mixed_f * lax.rsqrt(lax.optimization_barrier(jnp.mean(mixed_f * mixed_f, axis=-1, keepdims=True)) + norm_eps) * expert_norm_scale[None, :]).astype(jnp.bfloat16)
    pair_out = expert_outputs(normed, expert_index_table, expert_gate_weight, expert_up_weight, expert_down_weight)
    weights = jax.nn.sigmoid(expert_router_scores - expert_router_scores[:, ::-1])
    total = mixed_f + lax.optimization_barrier(jnp.sum(weights[:, :, None] * pair_out.astype(jnp.float32), axis=1))
    return total.astype(jnp.bfloat16)
```

```python
import jax
import jax.numpy as jnp
from jax import lax
from jax.experimental import pallas as pl
from jax.experimental.pallas import tpu as pltpu
from jax.sharding import PartitionSpec as P

HEAD_CHANNELS = 64
TOPK = 2


decay_factor = 0.6065306597126334
group_eps = 0.00064
norm_eps = 1e-06
key_eps = 1e-06
highest = lax.Precision.HIGHEST
block_len = 64
run_len = 8


def copy_for_each(shard, axis):
    copies = jnp.broadcast_to(shard, (lax.axis_size(axis), *shard.shape))
    return lax.all_to_all(copies, axis, split_axis=0, concat_axis=0, tiled=True)


def all_in_one(shard, axis):
    leaves = jax.tree.leaves(shard)
    order = sorted(range(len(leaves)), key=lambda k: -leaves[k].size)
    width = (1, *leaves[order[0]].shape)[-1]
    lines = [
        jnp.pad(leaves[k].reshape(-1), (0, -leaves[k].size % width)).reshape(-1, width)
        for k in order
    ]
    both, at, found = (copy_for_each(jnp.concatenate(lines), axis), 0, {})
    for k, line in zip(order, lines):
        share = both[:, at : at + len(line)].reshape(len(both), -1)
        found[k] = share[:, : leaves[k].size].reshape(-1, *leaves[k].shape)
        at += len(line)
    numbers = iter(range(len(leaves)))
    return jax.tree.map(lambda _: found[next(numbers)], shard)


def folded_in_pairs(pieces, combine):
    while len(jax.tree.leaves(pieces)[0]) > 1:
        pieces = jax.vmap(combine)(
            *(jax.tree.map(lambda part: part[side::2], pieces) for side in (0, 1))
        )
    return jax.tree.map(lambda part: part[0], pieces)


def entering_2(shard, axis, combine, identity):
    size, index = (lax.axis_size(axis), lax.axis_index(axis))
    passed = jnp.arange(size) < index

    def kept(part, zero, own):
        part = jnp.where(
            passed.reshape(-1, *(1 for _ in own.shape)),
            part.astype(own.dtype),
            jnp.asarray(zero, own.dtype),
        )
        return part

    pieces = all_in_one(
        jax.tree.map(
            lambda part, kind: part.astype(kind),
            shard,
            jax.tree.map(lambda a: jnp.bfloat16 if a.dtype == jnp.float32 else a.dtype, shard),
        ),
        axis,
    )
    return folded_in_pairs(jax.tree.map(kept, pieces, identity, shard), combine)


def matmul(left, right):
    return jnp.einsum("...ij,...jk->...ik", left, right, precision=highest)


def chain(earlier, later):
    return (matmul(earlier[0], later[0]), matmul(earlier[1], later[0]) + later[1])


seq_len = 256
chunk_len = 32
chunks = seq_len // chunk_len


def split_two(value):
    top = value.astype(jnp.bfloat16)
    return top, (value - top.astype(jnp.float32)).astype(jnp.bfloat16)


def dot_f32(left, right, dims=(((1,), (0,)), ((), ()))):
    return lax.dot_general(left, right, dims, preferred_element_type=jnp.float32)


def product(left, right):
    left_top, left_low = split_two(left)
    right_top, right_low = split_two(right)
    return dot_f32(
        jnp.concatenate([left_top, left_top, left_low], axis=1),
        jnp.concatenate([right_top, right_low, right_top], axis=0),
    )


def product_nt(left, right):
    left_top, left_low = split_two(left)
    right_top, right_low = split_two(right)
    return dot_f32(
        jnp.concatenate([left_top, left_top, left_low], axis=1),
        jnp.concatenate([right_top, right_low, right_top], axis=1),
        (((1,), (1,)), ((), ())),
    )


def sigmoid(value):
    return 1.0 / (1.0 + jnp.exp(-value))


def mixer_local(receptance, key_matrix, value_matrix, decay_input, decay_offset, head_decay, step_logits):
    key_vec = key_matrix.astype(jnp.float32)
    read_vec = receptance.astype(jnp.float32)
    log_decay = head_decay - decay_factor * sigmoid(decay_input.astype(jnp.float32) + decay_offset)
    learn = sigmoid(step_logits.astype(jnp.float32))
    unit = key_vec * lax.rsqrt(jnp.sum(key_vec * key_vec, axis=1, keepdims=True) + key_eps)
    write = unit * learn
    keyed = key_vec * learn

    row = lax.broadcasted_iota(jnp.int32, (seq_len, seq_len), 0)
    col = lax.broadcasted_iota(jnp.int32, (seq_len, seq_len), 1)
    same = (row >> 5) == (col >> 5)
    upto = same & (col <= row)
    before = same & (col < row)

    log_top, log_rest = split_two(log_decay)
    log_low = (log_decay - log_top.astype(jnp.float32) - log_rest.astype(jnp.float32)).astype(jnp.bfloat16)
    summed = dot_f32(
        jnp.where(upto, 1.0, 0.0).astype(jnp.bfloat16),
        jnp.concatenate([log_top, log_rest, log_low], axis=1),
    )
    total = summed[:, :64] + summed[:, 64:128] + summed[:, 128:192]
    by_chunk = total.reshape(chunks, chunk_len, HEAD_CHANNELS)
    middle = jnp.broadcast_to(by_chunk[:, chunk_len // 2 - 1 : chunk_len // 2], by_chunk.shape).reshape(total.shape)
    last = by_chunk[:, chunk_len - 1 : chunk_len]
    ending = jnp.broadcast_to(last, by_chunk.shape).reshape(total.shape)
    prior = total - log_decay

    up_scale = jnp.exp(middle - total)
    gram = product_nt(
        jnp.concatenate([-unit * jnp.exp(prior - middle), read_vec * jnp.exp(total - middle)], axis=0),
        jnp.concatenate([write * up_scale, keyed * up_scale], axis=0),
    )
    erase_write = jnp.where(before, gram[:seq_len, :seq_len], 0.0)
    erase_keyed = jnp.where(before, gram[:seq_len, seq_len:], 0.0)
    read_write = jnp.where(upto, gram[seq_len:, :seq_len], 0.0)
    read_keyed = jnp.where(upto, gram[seq_len:, seq_len:], 0.0)

    def below(width):
        return (
            ((row & (-2 * width)) == (col & (-2 * width)))
            & ((row & width) != 0)
            & ((col & width) == 0)
        )

    solved = jnp.where(row == col, 1.0, 0.0) + jnp.where(below(1), erase_write, 0.0)
    for width in (2, 4, 8, 16):
        solved = solved + product(solved, product(jnp.where(below(width), erase_write, 0.0), solved))

    stacked_top, stacked_low = split_two(jnp.concatenate([erase_keyed, read_keyed], axis=0))
    on_values = dot_f32(
        jnp.concatenate([stacked_top, stacked_low], axis=1),
        jnp.concatenate([value_matrix, value_matrix], axis=0),
    )
    erased = product(
        solved, jnp.concatenate([-unit * jnp.exp(prior), on_values[:seq_len]], axis=1)
    )
    shown = product(read_write, erased)
    seen = read_vec * jnp.exp(total) + shown[:, :64]
    own = shown[:, 64:] + on_values[seq_len:]

    tail_scale = jnp.exp(ending - total)
    wide_row = lax.broadcasted_iota(jnp.int32, (seq_len, chunks * 64), 0)
    wide_col = lax.broadcasted_iota(jnp.int32, (seq_len, chunks * 64), 1)
    in_block = (wide_row >> 5) == (wide_col >> 6)
    write_tail = jnp.where(in_block, jnp.concatenate([write * tail_scale] * chunks, axis=1), 0.0)
    keyed_tail = jnp.where(in_block, jnp.concatenate([keyed * tail_scale] * chunks, axis=1), 0.0)
    erased_t = jnp.transpose(erased)
    value_t = jnp.transpose(value_matrix.astype(jnp.float32)).astype(jnp.bfloat16)
    maps = product(erased_t, write_tail)
    keyed_top, keyed_low = split_two(keyed_tail)
    adds = maps[64:] + dot_f32(
        jnp.concatenate([value_t, value_t], axis=1),
        jnp.concatenate([keyed_top, keyed_low], axis=0),
    )
    small_row = lax.broadcasted_iota(jnp.int32, (64, 64), 0)
    small_col = lax.broadcasted_iota(jnp.int32, (64, 64), 1)
    eye = small_row == small_col

    through = [seen[:chunk_len]]
    local = [own[:chunk_len]]
    carried = None
    for c in range(chunks):
        step_map = maps[:64, c * 64 : (c + 1) * 64] + jnp.where(eye, jnp.exp(last[c]), 0.0)
        step_add = adds[:, c * 64 : (c + 1) * 64]
        if c == 0:
            carried = jnp.concatenate([step_map, step_add], axis=0)
        else:
            part = slice(c * chunk_len, (c + 1) * chunk_len)
            viewed = product_nt(seen[part], carried)
            through.append(viewed[:, :64])
            local.append(viewed[:, 64:] + own[part])
            moved = product(carried, step_map)
            carried = jnp.concatenate([moved[:64], moved[64:] + step_add], axis=0)
    return jnp.concatenate(through, axis=0), jnp.concatenate(local, axis=0), carried


def mixer_kernel(r_ref, k_ref, v_ref, d_ref, o_ref, h_ref, c_ref, through_ref, local_ref, final_ref):
    through, local, final = mixer_local(
        r_ref[...], k_ref[...], v_ref[...], d_ref[...], o_ref[...], h_ref[...], c_ref[...]
    )
    through_ref[...] = through
    local_ref[...] = local
    final_ref[...] = final


def run_mixer(*args):
    rows = jax.ShapeDtypeStruct((seq_len, HEAD_CHANNELS), jnp.float32)
    return pl.pallas_call(
        mixer_kernel,
        out_shape=(rows, rows, jax.ShapeDtypeStruct((128, 64), jnp.float32)),
    )(*args)


def finish(mixer_out, head_norm_scale, head_gate_rows):
    average = jnp.mean(mixer_out, axis=-1, keepdims=True)
    centred = mixer_out - average
    spread = jnp.mean(centred * centred, axis=-1, keepdims=True)
    normed = (centred * lax.rsqrt(spread + group_eps)).reshape(mixer_out.shape[0], -1)
    return (normed * head_norm_scale[None, :] * head_gate_rows.astype(jnp.float32)).astype(
        jnp.bfloat16
    )


MESH = pl.DeviceIdType.MESH
sub_rows = 16
subs = 4
half = 1024
width = 2048


def place(axis_0, axis_1):
    return (axis_0, axis_1)


def transfer(source, target, send, arrive, sp, tp):
    return pltpu.make_async_remote_copy(
        src_ref=source,
        dst_ref=target,
        send_sem=send,
        recv_sem=arrive,
        device_id=(sp, tp),
        device_id_type=MESH,
    )


def ranks_of(first, second):
    count = first.shape[0]
    lane = lax.broadcasted_iota(jnp.int32, (count, 128), 1).astype(jnp.float32)
    hit_0 = jnp.where(lane == first, 1.0, 0.0)
    hit_1 = jnp.where(lane == second, 1.0, 0.0)
    row = lax.broadcasted_iota(jnp.int32, (count, count), 0)
    col = lax.broadcasted_iota(jnp.int32, (count, count), 1)
    same = (row >> 4) == (col >> 4)
    earlier = dot_f32(
        jnp.where(same & (col < row), 1.0, 0.0).astype(jnp.bfloat16),
        jnp.concatenate([hit_0, hit_1], axis=1).astype(jnp.bfloat16),
    )
    every = dot_f32(jnp.where(same, 1.0, 0.0).astype(jnp.bfloat16), hit_0.astype(jnp.bfloat16))
    rank_0 = jnp.sum(earlier[:, :128] * hit_0, axis=1, keepdims=True)
    rank_1 = jnp.sum((earlier[:, 128:] + every) * hit_1, axis=1, keepdims=True)
    return first * 16.0 + rank_0, second * 16.0 + rank_1


def one_hot_rows(source_of):
    row = lax.broadcasted_iota(jnp.int32, (256, 256), 0)
    col = lax.broadcasted_iota(jnp.int32, (256, 256), 1)
    return jnp.where(col == source_of(row), 1.0, 0.0).astype(jnp.bfloat16)


def moe_kernel(
    normed_ref,
    mixed_ref,
    table_ref,
    gate_hbm,
    up_hbm,
    down_hbm,
    out_ref,
    gate_mat,
    up_mat,
    down_mat,
    outgoing,
    incoming,
    tables,
    codes,
    rows_all,
    gate_act,
    hidden_rows,
    mine_part,
    pair_out,
    pair_in,
    leave,
    back,
    sent_sum,
    got_sum,
    weight_sem,
    table_send,
    table_recv,
    spread_send,
    spread_recv,
    ring_send,
    ring_recv,
    twin_send,
    twin_recv,
    pair_send,
    pair_recv,
    back_send,
    back_recv,
    sum_send,
    sum_recv,
):
    sp, tp = lax.axis_index("sp"), lax.axis_index("tp")
    level, core = tp // 2, tp % 2
    twin = level * 2 + (1 - core)

    loads = [
        pltpu.make_async_copy(source.at[0], target, weight_sem.at[k])
        for k, (source, target) in enumerate(
            ((gate_hbm, gate_mat), (up_hbm, up_mat), (down_hbm, down_mat))
        )
    ]
    for load in loads:
        load.start()

    barrier = pltpu.get_barrier_semaphore()
    for j in range(1, 16):
        pl.semaphore_signal(barrier, inc=1, device_id=((sp + j) % 16, tp), device_id_type=MESH)
        pl.semaphore_signal(barrier, inc=1, device_id=(sp, (tp + j) % 16), device_id_type=MESH)

    own_table = table_ref[...]
    first, second = ranks_of(own_table[:, 0:1], own_table[:, 1:2])
    lane = lax.broadcasted_iota(jnp.int32, (16, 256), 1).astype(jnp.float32)
    spread = jnp.concatenate(
        [
            jnp.where((lane == first + 4.0 * q) | (lane == second + 4.0 * q), 1.0, 0.0)
            for q in range(4)
        ],
        axis=0,
    )
    normed = normed_ref[...]
    stacked = jnp.concatenate([normed[:, q * 512 : (q + 1) * 512] for q in range(4)], axis=0)
    outgoing[...] = dot_f32(
        jnp.transpose(spread).astype(jnp.bfloat16), stacked
    ).astype(jnp.bfloat16).reshape(16, 16, 512)

    pl.semaphore_wait(barrier, 30)

    pending = []
    for j in range(1, 16):
        other = (sp + j) % 16
        copy = transfer(
            outgoing.at[other], incoming.at[sp], spread_send.at[j], spread_recv.at[sp], other, tp
        )
        copy.start()
        pending.append(copy)
    incoming[sp] = outgoing[sp]
    for j in range(1, 16):
        other = (tp + j) % 16
        copy = transfer(table_ref, tables.at[tp], table_send.at[j], table_recv.at[tp], sp, other)
        copy.start()
        pending.append(copy)
    tables[tp] = own_table

    for j in range(1, 16):
        other = (sp + j) % 16
        transfer(
            outgoing.at[other], incoming.at[other], spread_send.at[j], spread_recv.at[other], other, tp
        ).wait_recv()
    regrouped = dot_f32(
        one_hot_rows(lambda j: ((j >> 2) & 15) * 16 + (j >> 6) * 4 + (j & 3)),
        incoming[...].reshape(256, 512),
    ).astype(jnp.bfloat16)
    rows_all[tp] = jnp.concatenate([regrouped[q * 64 : (q + 1) * 64] for q in range(4)], axis=1)

    following = (((level + 1) % 8) * 2 + core, ((level + 7) % 8) * 2 + core)

    def block_at(distance, way):
        if way == 0:
            return (level + 8 - distance) % 8
        return (level + distance) % 8

    def piece_of(index, sub):
        return rows_all.at[index, pl.ds(sub * sub_rows, sub_rows)]

    def arrival(distance, sub, way):
        return (distance - 1) * subs + sub if distance < 4 else 3 * subs + sub % 2

    def travels(distance, sub, way):
        return distance < 4 or (sub < 2) == (way == 0)

    def ring(index, sub, distance, way):
        slot = arrival(distance, sub, way)
        return transfer(
            piece_of(index, sub),
            piece_of(index, sub),
            ring_send.at[way, slot],
            ring_recv.at[way, slot],
            sp,
            following[way],
        )

    def twinned(index, sub, slot):
        return transfer(
            piece_of(index, sub), piece_of(index, sub), twin_send.at[slot], twin_recv.at[slot], sp, twin
        )

    def twin_slot(distance, sub, way):
        return subs + way * 14 + arrival(distance, sub, way)

    for sub in range(subs):
        for way in (0, 1):
            copy = ring(tp, sub, 1, way)
            copy.start()
            pending.append(copy)
        copy = twinned(tp, sub, sub)
        copy.start()
        pending.append(copy)

    def forward(distance, sub):
        for way in (0, 1):
            if not travels(distance, sub, way):
                continue
            index = block_at(distance, way) * 2 + core
            ring(index, sub, distance, way).wait_recv()
            if distance < 4 and travels(distance + 1, sub, way):
                copy = ring(index, sub, distance + 1, way)
                copy.start()
                pending.append(copy)
            copy = twinned(index, sub, twin_slot(distance, sub, way))
            copy.start()
            pending.append(copy)

    def await_twin(distance):
        if distance == 4:
            for sub in range(subs):
                twinned(twin, sub, sub).wait_recv()
        for sub in range(subs):
            for way in (0, 1):
                if travels(distance, sub, way):
                    index = block_at(distance, way) * 2 + (1 - core)
                    twinned(index, sub, twin_slot(distance, sub, way)).wait_recv()

    def members(distance):
        low = block_at(distance, 0) * 2 if distance < 4 else level * 2
        high = block_at(distance, 1) * 2
        return (low, low + 1, high, high + 1)

    for j in range(1, 16):
        other = (tp + j) % 16
        transfer(
            table_ref, tables.at[other], table_send.at[j], table_recv.at[other], sp, other
        ).wait_recv()
    every = tables[...].reshape(256, 128)
    first, second = ranks_of(every[:, 0:1], every[:, 1:2])
    gap = every[:, 3:4] - every[:, 2:3]
    wide_lane = lax.broadcasted_iota(jnp.int32, (256, 128), 1)
    codes[...] = jnp.where(
        wide_lane == 0,
        first,
        jnp.where(
            wide_lane == 1,
            second,
            jnp.where(wide_lane == 2, 1.0 / (1.0 + jnp.exp(gap)), 1.0 / (1.0 + jnp.exp(-gap))),
        ),
    ).reshape(16, 16, 128)
    for load in loads:
        load.wait()

    reorder = one_hot_rows(lambda j: ((j >> 2) & 3) * 64 + (j >> 4) * 4 + (j & 3))
    core_at = pl.multiple_of(core * half, half)
    twin_at = pl.multiple_of((1 - core) * half, half)

    def rows_in(distance):
        return jnp.concatenate([rows_all[index] for index in members(distance)], axis=0)

    def stage_gate(distance):
        gate_act[...] = dot_f32(rows_in(distance), gate_mat[...])

    def stage_up(distance):
        up_act = dot_f32(rows_in(distance), up_mat[...])
        gate = gate_act[...]
        hidden = (gate / (1.0 + jnp.exp(-gate)) * up_act).astype(jnp.bfloat16)
        hidden_rows[...] = dot_f32(reorder, hidden).astype(jnp.bfloat16)

    def pair(distance):
        at = distance - 1
        return transfer(
            pair_out.at[at], pair_in.at[at], pair_send.at[at], pair_recv.at[at], sp, twin
        )

    def stage_other(distance):
        pair_out[distance - 1] = dot_f32(
            hidden_rows[...], down_mat[:, pl.ds(twin_at, half)]
        ).astype(jnp.bfloat16)
        copy = pair(distance)
        copy.start()
        pending.append(copy)

    def stage_mine(distance):
        mine_part[...] = dot_f32(hidden_rows[...], down_mat[:, pl.ds(core_at, half)])

    def stage_return(distance):
        at = distance - 1
        pair(distance).wait_recv()
        leave[at] = (
            (mine_part[...] + pair_in[at].astype(jnp.float32)).astype(jnp.bfloat16).reshape(16, 16, half)
        )
        for j in range(1, 16):
            other = (sp + j) % 16
            copy = transfer(
                leave.at[at, other],
                back.at[at, sp],
                back_send.at[at, j],
                back_recv.at[at, sp],
                other,
                tp,
            )
            copy.start()
            pending.append(copy)
        back[at, sp] = leave[at, sp]

    def stage_combine(distance):
        at = distance - 1
        for j in range(1, 16):
            other = (sp + j) % 16
            transfer(
                leave.at[at, other],
                back.at[at, other],
                back_send.at[at, j],
                back_recv.at[at, other],
                other,
                tp,
            ).wait_recv()
        parts = []
        for place_in, index in enumerate(members(distance)):
            code = codes[index]
            parts.append(
                jnp.where(lane == code[:, 0:1] + 4.0 * place_in, code[:, 2:3], 0.0)
                + jnp.where(lane == code[:, 1:2] + 4.0 * place_in, code[:, 3:4], 0.0)
            )
        top, low = split_two(jnp.concatenate(parts, axis=0))
        returned = back[at].reshape(256, half)
        sent_sum[at] = (
            (dot_f32(top, returned) + dot_f32(low, returned)).astype(jnp.bfloat16).reshape(4, 16, half)
        )
        for place_in, index in enumerate(members(distance)):
            if distance == 4 and place_in < 2:
                continue
            copy = transfer(
                sent_sum.at[at, place_in],
                got_sum.at[tp],
                sum_send.at[at, place_in],
                sum_recv.at[tp],
                sp,
                index,
            )
            copy.start()
            pending.append(copy)
        if distance == 4:
            copy = transfer(
                sent_sum.at[at, 1 - core],
                got_sum.at[tp],
                sum_send.at[at, 0],
                sum_recv.at[tp],
                sp,
                twin,
            )
            copy.start()
            pending.append(copy)
            got_sum[tp] = sent_sum[at, core]

    for sub in range(subs):
        forward(1, sub)
    for distance in (1, 2, 3):
        await_twin(distance)
        stage_gate(distance)
        forward(distance + 1, 0)
        stage_up(distance)
        forward(distance + 1, 1)
        stage_other(distance)
        forward(distance + 1, 2)
        stage_mine(distance)
        forward(distance + 1, 3)
        stage_return(distance)
        if distance > 1:
            stage_combine(distance - 1)
    await_twin(4)
    stage_gate(4)
    stage_up(4)
    stage_other(4)
    stage_mine(4)
    stage_return(4)
    stage_combine(3)
    stage_combine(4)

    for j in range(1, 16):
        other = (tp + j) % 16
        transfer(
            sent_sum.at[0, 0], got_sum.at[other], sum_send.at[0, 0], sum_recv.at[other], sp, other
        ).wait_recv()
    for side in (0, 1):
        gathered = got_sum[side].astype(jnp.float32)
        for stage in range(1, 8):
            gathered = gathered + got_sum[2 * stage + side].astype(jnp.float32)
        cut = slice(side * half, (side + 1) * half)
        out_ref[:, cut] = (mixed_ref[:, cut].astype(jnp.float32) + gathered).astype(jnp.bfloat16)
    for copy in pending:
        copy.wait_send()


def run_moe(normed, mixed, table, gate, up, down):
    vmem = pl.BlockSpec(memory_space=pltpu.VMEM)
    hbm = pl.BlockSpec(memory_space=pl.ANY)
    dma = pltpu.SemaphoreType.DMA
    return pl.pallas_call(
        moe_kernel,
        out_shape=jax.ShapeDtypeStruct((16, width), jnp.bfloat16),
        in_specs=[vmem, vmem, vmem, hbm, hbm, hbm],
        out_specs=vmem,
        scratch_shapes=[
            pltpu.VMEM((width, 448), jnp.bfloat16),
            pltpu.VMEM((width, 448), jnp.bfloat16),
            pltpu.VMEM((448, width), jnp.bfloat16),
            pltpu.VMEM((16, 16, 512), jnp.bfloat16),
            pltpu.VMEM((16, 16, 512), jnp.bfloat16),
            pltpu.VMEM((16, 16, 128), jnp.float32),
            pltpu.VMEM((16, 16, 128), jnp.float32),
            pltpu.VMEM((16, 64, width), jnp.bfloat16),
            pltpu.VMEM((256, 448), jnp.float32),
            pltpu.VMEM((256, 448), jnp.bfloat16),
            pltpu.VMEM((256, half), jnp.float32),
            pltpu.VMEM((4, 256, half), jnp.bfloat16),
            pltpu.VMEM((4, 256, half), jnp.bfloat16),
            pltpu.VMEM((4, 16, 16, half), jnp.bfloat16),
            pltpu.VMEM((4, 16, 16, half), jnp.bfloat16),
            pltpu.VMEM((4, 4, 16, half), jnp.bfloat16),
            pltpu.VMEM((16, 16, half), jnp.bfloat16),
            dma((3,)),
            dma((16,)),
            dma((16,)),
            dma((16,)),
            dma((16,)),
            dma((2, 14)),
            dma((2, 14)),
            dma((32,)),
            dma((32,)),
            dma((4,)),
            dma((4,)),
            dma((4, 16)),
            dma((4, 16)),
            dma((4, 4)),
            dma((16,)),
        ],
        compiler_params=pltpu.CompilerParams(
            collective_id=1, has_side_effects=True, vmem_limit_bytes=56 * 1024 * 1024
        ),
    )(normed, mixed, table, gate, up, down)


def shards(
    receptance,
    key_matrix,
    value_matrix,
    decay_input_term,
    decay_channel_offset,
    head_log_decay,
    context_step_logits,
    head_gate_rows,
    head_norm_scale,
    mixer_output_weight,
    residual,
    expert_norm_scale,
    expert_index_table,
    expert_router_scores,
    expert_gate_weight,
    expert_up_weight,
    expert_down_weight,
):
    through, local_out, final = run_mixer(
        receptance,
        key_matrix,
        value_matrix,
        decay_input_term,
        decay_channel_offset.reshape(1, -1),
        head_log_decay,
        context_step_logits,
    )
    through, local_out = through[:, None, :], local_out[:, None, :]
    final = (final[None, :64], final[None, 64:])
    start_map = jnp.broadcast_to(jnp.eye(final[0].shape[1], dtype=jnp.float32), final[0].shape)
    entering = entering_2(final, "sp", chain, (start_map, jnp.zeros_like(final[1])))
    mixer_out = local_out + jnp.einsum("hij,thj->thi", entering[1], through, precision=highest)
    attended = finish(mixer_out, head_norm_scale, head_gate_rows)
    row_count = residual.shape[0]
    token_rows = lax.all_to_all(attended, "tp", split_axis=0, concat_axis=1, tiled=True)
    projected = jnp.dot(token_rows, mixer_output_weight, preferred_element_type=jnp.float32)
    mixed = (residual.astype(jnp.float32) + projected).astype(jnp.bfloat16)
    mixed_f = mixed.astype(jnp.float32)
    normed = (
        mixed_f
        * lax.rsqrt(jnp.mean(mixed_f * mixed_f, axis=-1, keepdims=True) + norm_eps)
        * expert_norm_scale[None, :]
    ).astype(jnp.bfloat16)
    table = jnp.concatenate(
        [
            expert_index_table.astype(jnp.float32),
            expert_router_scores,
            jnp.zeros((row_count, 124), jnp.float32),
        ],
        axis=1,
    )
    return run_moe(normed, mixed, table, expert_gate_weight, expert_up_weight, expert_down_weight)


def solution(mesh):
    return jax.shard_map(
        shards,
        mesh=mesh,
        in_specs=(
            P("sp", "tp"),
            P("sp", "tp"),
            P("sp", "tp"),
            P("sp", "tp"),
            P("tp"),
            P("sp", "tp"),
            P("sp", "tp"),
            P("sp", "tp"),
            P("tp"),
            P(),
            P(("sp", "tp"), None),
            P(),
            P(("sp", "tp"), None),
            P(("sp", "tp"), None),
            P("sp", None, "tp"),
            P("sp", None, "tp"),
            P("sp", "tp", None),
        ),
        out_specs=P(("sp", "tp"), None),
        check_vma=False,
    )
```

```python
import jax
import jax.numpy as jnp
from jax import lax
from jax.experimental import pallas as pl
from jax.experimental.pallas import tpu as pltpu
from jax.sharding import PartitionSpec as P

HEAD_CHANNELS = 64

decay_factor = 0.6065306597126334
group_eps = 0.00064
norm_eps = 1e-06
key_eps = 1e-06
seq_len = 256
chunk_len = 32
chunks = seq_len // chunk_len


def split_two(value):
    top = value.astype(jnp.bfloat16)
    return top, (value - top.astype(jnp.float32)).astype(jnp.bfloat16)


def dot_f32(left, right, dims=(((1,), (0,)), ((), ()))):
    return lax.dot_general(left, right, dims, preferred_element_type=jnp.float32)


def product(left, right):
    left_top, left_low = split_two(left)
    right_top, right_low = split_two(right)
    return dot_f32(
        jnp.concatenate([left_top, left_top, left_low], axis=1),
        jnp.concatenate([right_top, right_low, right_top], axis=0),
    )


def product_nt(left, right):
    left_top, left_low = split_two(left)
    right_top, right_low = split_two(right)
    return dot_f32(
        jnp.concatenate([left_top, left_top, left_low], axis=1),
        jnp.concatenate([right_top, right_low, right_top], axis=1),
        (((1,), (1,)), ((), ())),
    )


def sigmoid(value):
    return 1.0 / (1.0 + jnp.exp(-value))


def turned(value):
    return jnp.transpose(value.astype(jnp.float32))


def mixer_local(receptance, key_matrix, value_t, decay_input, decay_offset, head_decay, step_logits):
    read_vec, key_vec = turned(receptance), turned(key_matrix)
    value_matrix = turned(value_t).astype(jnp.bfloat16)
    head_column = turned(jnp.broadcast_to(head_decay, (8, seq_len)))[:, 0:1]
    log_decay = head_column - decay_factor * sigmoid(turned(decay_input) + decay_offset)
    learn = turned(sigmoid(step_logits.astype(jnp.float32)))
    unit = key_vec * lax.rsqrt(jnp.sum(key_vec * key_vec, axis=1, keepdims=True) + key_eps)
    write = unit * learn
    keyed = key_vec * learn

    row = lax.broadcasted_iota(jnp.int32, (seq_len, seq_len), 0)
    col = lax.broadcasted_iota(jnp.int32, (seq_len, seq_len), 1)
    same = (row >> 5) == (col >> 5)
    upto = same & (col <= row)
    before = same & (col < row)

    log_top, log_rest = split_two(log_decay)
    log_low = (log_decay - log_top.astype(jnp.float32) - log_rest.astype(jnp.float32)).astype(jnp.bfloat16)
    summed = dot_f32(
        jnp.where(upto, 1.0, 0.0).astype(jnp.bfloat16),
        jnp.concatenate([log_top, log_rest, log_low], axis=1),
    )
    total = summed[:, :64] + summed[:, 64:128] + summed[:, 128:192]
    by_chunk = total.reshape(chunks, chunk_len, HEAD_CHANNELS)
    middle = jnp.broadcast_to(by_chunk[:, chunk_len // 2 - 1 : chunk_len // 2], by_chunk.shape).reshape(total.shape)
    last = by_chunk[:, chunk_len - 1 : chunk_len]
    ending = jnp.broadcast_to(last, by_chunk.shape).reshape(total.shape)
    prior = total - log_decay

    up_scale = jnp.exp(middle - total)
    gram = product_nt(
        jnp.concatenate([-unit * jnp.exp(prior - middle), read_vec * jnp.exp(total - middle)], axis=0),
        jnp.concatenate([write * up_scale, keyed * up_scale], axis=0),
    )
    erase_write = jnp.where(before, gram[:seq_len, :seq_len], 0.0)
    erase_keyed = jnp.where(before, gram[:seq_len, seq_len:], 0.0)
    read_write = jnp.where(upto, gram[seq_len:, :seq_len], 0.0)
    read_keyed = jnp.where(upto, gram[seq_len:, seq_len:], 0.0)

    def below(width):
        return (
            ((row & (-2 * width)) == (col & (-2 * width)))
            & ((row & width) != 0)
            & ((col & width) == 0)
        )

    solved = jnp.where(row == col, 1.0, 0.0) + jnp.where(below(1), erase_write, 0.0)
    for width in (2, 4, 8, 16):
        solved = solved + product(solved, product(jnp.where(below(width), erase_write, 0.0), solved))

    stacked_top, stacked_low = split_two(jnp.concatenate([erase_keyed, read_keyed], axis=0))
    on_values = dot_f32(
        jnp.concatenate([stacked_top, stacked_low], axis=1),
        jnp.concatenate([value_matrix, value_matrix], axis=0),
    )
    erased = product(
        solved, jnp.concatenate([-unit * jnp.exp(prior), on_values[:seq_len]], axis=1)
    )
    shown = product(read_write, erased)
    seen = read_vec * jnp.exp(total) + shown[:, :64]
    own = shown[:, 64:] + on_values[seq_len:]

    tail_scale = jnp.exp(ending - total)
    wide_row = lax.broadcasted_iota(jnp.int32, (seq_len, chunks * 64), 0)
    wide_col = lax.broadcasted_iota(jnp.int32, (seq_len, chunks * 64), 1)
    in_block = (wide_row >> 5) == (wide_col >> 6)
    write_tail = jnp.where(in_block, jnp.concatenate([write * tail_scale] * chunks, axis=1), 0.0)
    keyed_tail = jnp.where(in_block, jnp.concatenate([keyed * tail_scale] * chunks, axis=1), 0.0)
    erased_t = jnp.transpose(erased)
    maps = product(erased_t, write_tail)
    keyed_top, keyed_low = split_two(keyed_tail)
    adds = maps[64:] + dot_f32(
        jnp.concatenate([value_t, value_t], axis=1),
        jnp.concatenate([keyed_top, keyed_low], axis=0),
    )
    small_row = lax.broadcasted_iota(jnp.int32, (64, 64), 0)
    small_col = lax.broadcasted_iota(jnp.int32, (64, 64), 1)
    eye = small_row == small_col

    through = [seen[:chunk_len]]
    local = [own[:chunk_len]]
    carried = None
    for c in range(chunks):
        step_map = maps[:64, c * 64 : (c + 1) * 64] + jnp.where(eye, jnp.exp(last[c]), 0.0)
        step_add = adds[:, c * 64 : (c + 1) * 64]
        if c == 0:
            carried = jnp.concatenate([step_map, step_add], axis=0)
        else:
            part = slice(c * chunk_len, (c + 1) * chunk_len)
            viewed = product_nt(seen[part], carried)
            through.append(viewed[:, :64])
            local.append(viewed[:, 64:] + own[part])
            moved = product(carried, step_map)
            carried = jnp.concatenate([moved[:64], moved[64:] + step_add], axis=0)
    return jnp.concatenate(through, axis=0), jnp.concatenate(local, axis=0), carried


MESH = pl.DeviceIdType.MESH
sub_rows = 16
subs = 4
half = 1024
width = 2048


def transfer(source, target, send, arrive, sp, tp):
    return pltpu.make_async_remote_copy(
        src_ref=source,
        dst_ref=target,
        send_sem=send,
        recv_sem=arrive,
        device_id=(sp, tp),
        device_id_type=MESH,
    )


def ranks_of(first, second):
    count = first.shape[0]
    lane = lax.broadcasted_iota(jnp.int32, (count, 128), 1).astype(jnp.float32)
    hit_0 = jnp.where(lane == first, 1.0, 0.0)
    hit_1 = jnp.where(lane == second, 1.0, 0.0)
    row = lax.broadcasted_iota(jnp.int32, (count, count), 0)
    col = lax.broadcasted_iota(jnp.int32, (count, count), 1)
    same = (row >> 4) == (col >> 4)
    earlier = dot_f32(
        jnp.where(same & (col < row), 1.0, 0.0).astype(jnp.bfloat16),
        jnp.concatenate([hit_0, hit_1], axis=1).astype(jnp.bfloat16),
    )
    every = dot_f32(jnp.where(same, 1.0, 0.0).astype(jnp.bfloat16), hit_0.astype(jnp.bfloat16))
    rank_0 = jnp.sum(earlier[:, :128] * hit_0, axis=1, keepdims=True)
    rank_1 = jnp.sum((earlier[:, 128:] + every) * hit_1, axis=1, keepdims=True)
    return first * 16.0 + rank_0, second * 16.0 + rank_1


def one_hot_rows(source_of):
    row = lax.broadcasted_iota(jnp.int32, (256, 256), 0)
    col = lax.broadcasted_iota(jnp.int32, (256, 256), 1)
    return jnp.where(col == source_of(row), 1.0, 0.0).astype(jnp.bfloat16)


def fold_states(states):
    nodes = []
    for i in range(8):
        early, late = states[2 * i], states[2 * i + 1]
        stacked = jnp.concatenate([early[:, :64], early[:, 64:]], axis=0)
        moved = dot_f32(stacked, late[:, :64])
        nodes.append((moved[:64], moved[64:] + late[:, 64:].astype(jnp.float32)))
    while len(nodes) > 1:
        joined = []
        for i in range(0, len(nodes), 2):
            (early_map, early_state), (late_map, late_state) = nodes[i], nodes[i + 1]
            if i == 0:
                joined.append((None, product(early_state, late_map) + late_state))
            else:
                moved = product(jnp.concatenate([early_map, early_state], axis=0), late_map)
                joined.append((moved[:64], moved[64:] + late_state))
        nodes = joined
    return nodes[0][1]


def finish(mixer_out, head_norm_scale, head_gate_rows):
    average = jnp.mean(mixer_out, axis=1, keepdims=True)
    centred = mixer_out - average
    spread = jnp.mean(centred * centred, axis=1, keepdims=True)
    return centred * lax.rsqrt(spread + group_eps) * head_norm_scale * head_gate_rows


def layer_kernel(
    r_ref,
    k_ref,
    v_ref,
    d_ref,
    o_ref,
    h_ref,
    c_ref,
    g_ref,
    scale_ref,
    residual_ref,
    norm_ref,
    index_ref,
    score_ref,
    mix_hbm,
    gate_hbm,
    up_hbm,
    down_hbm,
    out_ref,
    mix_mat,
    gate_mat,
    up_mat,
    down_mat,
    through_ref,
    local_ref,
    state_out,
    states,
    heads_out,
    heads_in,
    mixed_ref,
    table_ref,
    outgoing,
    incoming,
    tables,
    codes,
    rows_all,
    gate_act,
    hidden_rows,
    mine_part,
    pair_out,
    pair_in,
    leave,
    back,
    sent_sum,
    got_sum,
    weight_sem,
    state_send,
    state_recv,
    heads_send,
    heads_recv,
    table_send,
    table_recv,
    spread_send,
    spread_recv,
    ring_send,
    ring_recv,
    twin_send,
    twin_recv,
    pair_send,
    pair_recv,
    back_send,
    back_recv,
    sum_send,
    sum_recv,
):
    sp, tp = lax.axis_index("sp"), lax.axis_index("tp")
    level, core = tp // 2, tp % 2
    twin = level * 2 + (1 - core)

    loads = [
        pltpu.make_async_copy(source, target, weight_sem.at[k])
        for k, (source, target) in enumerate(
            (
                (mix_hbm, mix_mat),
                (gate_hbm.at[0], gate_mat),
                (up_hbm.at[0], up_mat),
                (down_hbm.at[0], down_mat),
            )
        )
    ]
    for load in loads:
        load.start()

    start_row = lax.broadcasted_iota(jnp.int32, (16, 64, 128), 1)
    start_col = lax.broadcasted_iota(jnp.int32, (16, 64, 128), 2)
    states[...] = jnp.where(start_row == start_col, 1.0, 0.0).astype(jnp.bfloat16)

    barrier = pltpu.get_barrier_semaphore()
    for j in range(1, 16):
        pl.semaphore_signal(barrier, inc=1, device_id=((sp + j) % 16, tp), device_id_type=MESH)
        pl.semaphore_signal(barrier, inc=1, device_id=(sp, (tp + j) % 16), device_id_type=MESH)

    through, local, final = mixer_local(
        r_ref[...], k_ref[...], v_ref[...], d_ref[...], o_ref[...], h_ref[...], c_ref[...]
    )
    state_out[...] = jnp.concatenate([final[:64], final[64:]], axis=1).astype(jnp.bfloat16)
    through_ref[...] = through
    local_ref[...] = local
    table_ref[...] = jnp.concatenate(
        [
            jnp.transpose(
                jnp.concatenate(
                    [
                        jnp.concatenate(
                            [index_ref[...].astype(jnp.float32), score_ref[...]], axis=0
                        ),
                        jnp.zeros((4, 112), jnp.float32),
                    ],
                    axis=1,
                )
            )[:16],
            jnp.zeros((16, 124), jnp.float32),
        ],
        axis=1,
    )

    pl.semaphore_wait(barrier, 30)

    pending = []

    def state_copy(j, source, target):
        return transfer(
            state_out, states.at[source], state_send.at[j], state_recv.at[source], target, tp
        )

    for j in range(1, 16):

        @pl.when(sp + j < 16)
        def _():
            state_copy(j, sp, sp + j).start()

    for j in range(1, 16):
        other = (tp + j) % 16
        copy = transfer(table_ref, tables.at[tp], table_send.at[j], table_recv.at[tp], sp, other)
        copy.start()
        pending.append(copy)
    tables[tp] = table_ref[...]

    own_table = table_ref[...]
    first, second = ranks_of(own_table[:, 0:1], own_table[:, 1:2])
    lane = lax.broadcasted_iota(jnp.int32, (16, 256), 1).astype(jnp.float32)
    spread = jnp.transpose(
        jnp.concatenate(
            [
                jnp.where((lane == first + 4.0 * q) | (lane == second + 4.0 * q), 1.0, 0.0)
                for q in range(4)
            ],
            axis=0,
        )
    ).astype(jnp.bfloat16)

    for j in range(1, 16):

        @pl.when(sp - j >= 0)
        def _():
            state_copy(j, sp - j, sp).wait_recv()

    entering = fold_states(states[...])
    attended = finish(
        local_ref[...] + product_nt(through_ref[...], entering), scale_ref[...], turned(g_ref[...])
    )
    both = jnp.concatenate([attended, attended], axis=1)
    side_lane = lax.broadcasted_iota(jnp.int32, (seq_len, 128), 1) // 64
    heads_out[...] = jnp.where(side_lane == core, both, 0.0).astype(jnp.bfloat16).reshape(16, 16, 128)
    for j in range(1, 16):
        other = (tp + j) % 16
        copy = transfer(
            heads_out.at[other], heads_in.at[tp], heads_send.at[j], heads_recv.at[tp], sp, other
        )
        copy.start()
        pending.append(copy)
    heads_in[tp] = heads_out[tp]

    for j in range(1, 16):
        other = (tp + j) % 16
        transfer(
            table_ref, tables.at[other], table_send.at[j], table_recv.at[other], sp, other
        ).wait_recv()
    every = tables[...].reshape(256, 128)
    all_first, all_second = ranks_of(every[:, 0:1], every[:, 1:2])
    gap = every[:, 3:4] - every[:, 2:3]
    wide_lane = lax.broadcasted_iota(jnp.int32, (256, 128), 1)
    codes[...] = jnp.where(
        wide_lane == 0,
        all_first,
        jnp.where(
            wide_lane == 1,
            all_second,
            jnp.where(wide_lane == 2, 1.0 / (1.0 + jnp.exp(gap)), 1.0 / (1.0 + jnp.exp(-gap))),
        ),
    ).reshape(16, 16, 128)
    for load in loads:
        load.wait()

    for j in range(1, 16):
        other = (tp + j) % 16
        transfer(
            heads_out.at[other], heads_in.at[other], heads_send.at[j], heads_recv.at[other], sp, other
        ).wait_recv()
    tokens = jnp.concatenate([heads_in[2 * i] + heads_in[2 * i + 1] for i in range(8)], axis=1)
    mixed_f = (
        (residual_ref[...].astype(jnp.float32) + dot_f32(tokens, mix_mat[...]))
        .astype(jnp.bfloat16)
        .astype(jnp.float32)
    )
    mixed_ref[...] = mixed_f
    normed = (
        mixed_f
        * lax.rsqrt(jnp.mean(mixed_f * mixed_f, axis=1, keepdims=True) + norm_eps)
        * norm_ref[...]
    ).astype(jnp.bfloat16)
    stacked = jnp.concatenate([normed[:, q * 512 : (q + 1) * 512] for q in range(4)], axis=0)
    outgoing[...] = dot_f32(spread, stacked).astype(jnp.bfloat16).reshape(16, 16, 512)
    for j in range(1, 16):
        other = (sp + j) % 16
        copy = transfer(
            outgoing.at[other], incoming.at[sp], spread_send.at[j], spread_recv.at[sp], other, tp
        )
        copy.start()
        pending.append(copy)
    incoming[sp] = outgoing[sp]

    for j in range(1, 16):
        other = (sp + j) % 16
        transfer(
            outgoing.at[other], incoming.at[other], spread_send.at[j], spread_recv.at[other], other, tp
        ).wait_recv()
    regrouped = dot_f32(
        one_hot_rows(lambda j: ((j >> 2) & 15) * 16 + (j >> 6) * 4 + (j & 3)),
        incoming[...].reshape(256, 512),
    ).astype(jnp.bfloat16)
    rows_all[tp] = jnp.concatenate([regrouped[q * 64 : (q + 1) * 64] for q in range(4)], axis=1)

    following = (((level + 1) % 8) * 2 + core, ((level + 7) % 8) * 2 + core)

    def block_at(distance, way):
        if way == 0:
            return (level + 8 - distance) % 8
        return (level + distance) % 8

    def piece_of(index, sub):
        return rows_all.at[index, pl.ds(sub * sub_rows, sub_rows)]

    def arrival(distance, sub, way):
        return (distance - 1) * subs + sub if distance < 4 else 3 * subs + sub % 2

    def travels(distance, sub, way):
        return distance < 4 or (sub < 2) == (way == 0)

    def ring(index, sub, distance, way):
        slot = arrival(distance, sub, way)
        return transfer(
            piece_of(index, sub),
            piece_of(index, sub),
            ring_send.at[way, slot],
            ring_recv.at[way, slot],
            sp,
            following[way],
        )

    def twinned(index, sub, slot):
        return transfer(
            piece_of(index, sub), piece_of(index, sub), twin_send.at[slot], twin_recv.at[slot], sp, twin
        )

    def twin_slot(distance, sub, way):
        return subs + way * 14 + arrival(distance, sub, way)

    for sub in range(subs):
        for way in (0, 1):
            copy = ring(tp, sub, 1, way)
            copy.start()
            pending.append(copy)
        copy = twinned(tp, sub, sub)
        copy.start()
        pending.append(copy)

    def forward(distance, sub):
        for way in (0, 1):
            if not travels(distance, sub, way):
                continue
            index = block_at(distance, way) * 2 + core
            ring(index, sub, distance, way).wait_recv()
            if distance < 4 and travels(distance + 1, sub, way):
                copy = ring(index, sub, distance + 1, way)
                copy.start()
                pending.append(copy)
            copy = twinned(index, sub, twin_slot(distance, sub, way))
            copy.start()
            pending.append(copy)

    def await_twin(distance):
        if distance == 4:
            for sub in range(subs):
                twinned(twin, sub, sub).wait_recv()
        for sub in range(subs):
            for way in (0, 1):
                if travels(distance, sub, way):
                    index = block_at(distance, way) * 2 + (1 - core)
                    twinned(index, sub, twin_slot(distance, sub, way)).wait_recv()

    def members(distance):
        low = block_at(distance, 0) * 2 if distance < 4 else level * 2
        high = block_at(distance, 1) * 2
        return (low, low + 1, high, high + 1)

    reorder = one_hot_rows(lambda j: ((j >> 2) & 3) * 64 + (j >> 4) * 4 + (j & 3))
    core_at = pl.multiple_of(core * half, half)
    twin_at = pl.multiple_of((1 - core) * half, half)

    def rows_in(distance):
        return jnp.concatenate([rows_all[index] for index in members(distance)], axis=0)

    def stage_gate(distance):
        gate_act[...] = dot_f32(rows_in(distance), gate_mat[...], (((1,), (1,)), ((), ())))

    def stage_up(distance):
        up_act = dot_f32(rows_in(distance), up_mat[...], (((1,), (1,)), ((), ())))
        gate = gate_act[...]
        hidden = (gate / (1.0 + jnp.exp(-gate)) * up_act).astype(jnp.bfloat16)
        hidden_rows[...] = dot_f32(reorder, hidden).astype(jnp.bfloat16)

    def pair(distance):
        at = distance - 1
        return transfer(
            pair_out.at[at], pair_in.at[at], pair_send.at[at], pair_recv.at[at], sp, twin
        )

    def stage_other(distance):
        pair_out[distance - 1] = dot_f32(
            hidden_rows[...], down_mat[:, pl.ds(twin_at, half)]
        ).astype(jnp.bfloat16)
        copy = pair(distance)
        copy.start()
        pending.append(copy)

    def stage_mine(distance):
        mine_part[...] = dot_f32(hidden_rows[...], down_mat[:, pl.ds(core_at, half)])

    def stage_return(distance):
        at = distance - 1
        pair(distance).wait_recv()
        leave[at] = (
            (mine_part[...] + pair_in[at].astype(jnp.float32)).astype(jnp.bfloat16).reshape(16, 16, half)
        )
        for j in range(1, 16):
            other = (sp + j) % 16
            copy = transfer(
                leave.at[at, other],
                back.at[at, sp],
                back_send.at[at, j],
                back_recv.at[at, sp],
                other,
                tp,
            )
            copy.start()
            pending.append(copy)
        back[at, sp] = leave[at, sp]

    def stage_combine(distance):
        at = distance - 1
        for j in range(1, 16):
            other = (sp + j) % 16
            transfer(
                leave.at[at, other],
                back.at[at, other],
                back_send.at[at, j],
                back_recv.at[at, other],
                other,
                tp,
            ).wait_recv()
        parts = []
        for place_in, index in enumerate(members(distance)):
            code = codes[index]
            parts.append(
                jnp.where(lane == code[:, 0:1] + 4.0 * place_in, code[:, 2:3], 0.0)
                + jnp.where(lane == code[:, 1:2] + 4.0 * place_in, code[:, 3:4], 0.0)
            )
        top, low = split_two(jnp.concatenate(parts, axis=0))
        returned = back[at].reshape(256, half)
        sent_sum[at] = (
            (dot_f32(top, returned) + dot_f32(low, returned)).astype(jnp.bfloat16).reshape(4, 16, half)
        )
        for place_in, index in enumerate(members(distance)):
            if distance == 4 and place_in < 2:
                continue
            copy = transfer(
                sent_sum.at[at, place_in],
                got_sum.at[tp],
                sum_send.at[at, place_in],
                sum_recv.at[tp],
                sp,
                index,
            )
            copy.start()
            pending.append(copy)
        if distance == 4:
            copy = transfer(
                sent_sum.at[at, 1 - core],
                got_sum.at[tp],
                sum_send.at[at, 0],
                sum_recv.at[tp],
                sp,
                twin,
            )
            copy.start()
            pending.append(copy)
            got_sum[tp] = sent_sum[at, core]

    for sub in range(subs):
        forward(1, sub)
    for distance in (1, 2, 3):
        await_twin(distance)
        stage_gate(distance)
        forward(distance + 1, 0)
        stage_up(distance)
        forward(distance + 1, 1)
        stage_other(distance)
        forward(distance + 1, 2)
        stage_mine(distance)
        forward(distance + 1, 3)
        stage_return(distance)
        if distance > 1:
            stage_combine(distance - 1)
    await_twin(4)
    stage_gate(4)
    stage_up(4)
    stage_other(4)
    stage_mine(4)
    stage_return(4)
    stage_combine(3)
    stage_combine(4)

    for j in range(1, 16):
        other = (tp + j) % 16
        transfer(
            sent_sum.at[0, 0], got_sum.at[other], sum_send.at[0, 0], sum_recv.at[other], sp, other
        ).wait_recv()
    for side in (0, 1):
        gathered = got_sum[side].astype(jnp.float32)
        for stage in range(1, 8):
            gathered = gathered + got_sum[2 * stage + side].astype(jnp.float32)
        cut = slice(side * half, (side + 1) * half)
        out_ref[:, cut] = (mixed_ref[:, cut] + gathered).astype(jnp.bfloat16)
    for copy in pending:
        copy.wait_send()
    for j in range(1, 16):

        @pl.when(sp + j < 16)
        def _():
            state_copy(j, sp, sp + j).wait_send()


def shards(
    receptance,
    key_matrix,
    value_matrix,
    decay_input_term,
    decay_channel_offset,
    head_log_decay,
    context_step_logits,
    head_gate_rows,
    head_norm_scale,
    mixer_output_weight,
    residual,
    expert_norm_scale,
    expert_index_table,
    expert_router_scores,
    expert_gate_weight,
    expert_up_weight,
    expert_down_weight,
):
    vmem = pl.BlockSpec(memory_space=pltpu.VMEM)
    hbm = pl.BlockSpec(memory_space=pl.ANY)
    dma = pltpu.SemaphoreType.DMA
    b16, f32 = jnp.bfloat16, jnp.float32
    return pl.pallas_call(
        layer_kernel,
        out_shape=jax.ShapeDtypeStruct((16, width), jnp.bfloat16),
        in_specs=[vmem] * 13 + [hbm] * 4,
        out_specs=vmem,
        scratch_shapes=[
            pltpu.VMEM((1024, width), b16),
            pltpu.VMEM((448, width), b16),
            pltpu.VMEM((448, width), b16),
            pltpu.VMEM((448, width), b16),
            pltpu.VMEM((seq_len, 64), f32),
            pltpu.VMEM((seq_len, 64), f32),
            pltpu.VMEM((64, 128), b16),
            pltpu.VMEM((16, 64, 128), b16),
            pltpu.VMEM((16, 16, 128), b16),
            pltpu.VMEM((16, 16, 128), b16),
            pltpu.VMEM((16, width), f32),
            pltpu.VMEM((16, 128), f32),
            pltpu.VMEM((16, 16, 512), b16),
            pltpu.VMEM((16, 16, 512), b16),
            pltpu.VMEM((16, 16, 128), f32),
            pltpu.VMEM((16, 16, 128), f32),
            pltpu.VMEM((16, 64, width), b16),
            pltpu.VMEM((256, 448), f32),
            pltpu.VMEM((256, 448), b16),
            pltpu.VMEM((256, half), f32),
            pltpu.VMEM((4, 256, half), b16),
            pltpu.VMEM((4, 256, half), b16),
            pltpu.VMEM((4, 16, 16, half), b16),
            pltpu.VMEM((4, 16, 16, half), b16),
            pltpu.VMEM((4, 4, 16, half), b16),
            pltpu.VMEM((16, 16, half), b16),
            dma((4,)),
        ]
        + [dma((16,))] * 8
        + [dma((2, 14))] * 2
        + [dma((32,))] * 2
        + [dma((4,))] * 2
        + [dma((4, 16))] * 2
        + [dma((4, 4)), dma((16,))],
        compiler_params=pltpu.CompilerParams(
            collective_id=1, has_side_effects=True, vmem_limit_bytes=56 * 1024 * 1024
        ),
    )(
        receptance.T,
        key_matrix.T,
        value_matrix.T,
        decay_input_term.T,
        decay_channel_offset.reshape(1, -1),
        head_log_decay.T,
        context_step_logits.T,
        head_gate_rows.T,
        head_norm_scale.reshape(1, -1),
        residual,
        expert_norm_scale.reshape(1, -1),
        expert_index_table.T,
        expert_router_scores.T,
        mixer_output_weight,
        jnp.swapaxes(expert_gate_weight, 1, 2),
        jnp.swapaxes(expert_up_weight, 1, 2),
        expert_down_weight,
    )


def solution(mesh):
    return jax.shard_map(
        shards,
        mesh=mesh,
        in_specs=(
            P("sp", "tp"),
            P("sp", "tp"),
            P("sp", "tp"),
            P("sp", "tp"),
            P("tp"),
            P("sp", "tp"),
            P("sp", "tp"),
            P("sp", "tp"),
            P("tp"),
            P(),
            P(("sp", "tp"), None),
            P(),
            P(("sp", "tp"), None),
            P(("sp", "tp"), None),
            P("sp", None, "tp"),
            P("sp", None, "tp"),
            P("sp", "tp", None),
        ),
        out_specs=P(("sp", "tp"), None),
        check_vma=False,
    )
```

```python
import jax
import jax.numpy as jnp
from jax import lax
from jax.experimental import pallas as pl
from jax.experimental.pallas import tpu as pltpu
from jax.sharding import PartitionSpec as P

HEAD_CHANNELS = 64

decay_factor = 0.6065306597126334
group_eps = 0.00064
norm_eps = 1e-06
key_eps = 1e-06
seq_len = 256
chunk_len = 32
chunks = seq_len // chunk_len


def split_two(value):
    top = value.astype(jnp.bfloat16)
    return top, (value - top.astype(jnp.float32)).astype(jnp.bfloat16)


def dot_f32(left, right, dims=(((1,), (0,)), ((), ()))):
    return lax.dot_general(left, right, dims, preferred_element_type=jnp.float32)


def product(left, right):
    left_top, left_low = split_two(left)
    right_top, right_low = split_two(right)
    return dot_f32(
        jnp.concatenate([left_top, left_top, left_low], axis=1),
        jnp.concatenate([right_top, right_low, right_top], axis=0),
    )


def product_nt(left, right):
    left_top, left_low = split_two(left)
    right_top, right_low = split_two(right)
    return dot_f32(
        jnp.concatenate([left_top, left_top, left_low], axis=1),
        jnp.concatenate([right_top, right_low, right_top], axis=1),
        (((1,), (1,)), ((), ())),
    )


def sigmoid(value):
    return 1.0 / (1.0 + jnp.exp(-value))


def turned(value):
    return jnp.transpose(value.astype(jnp.float32))


def mixer_local(receptance, key_matrix, value_t, decay_input, decay_offset, head_decay, step_logits):
    read_vec, key_vec = turned(receptance), turned(key_matrix)
    value_matrix = turned(value_t).astype(jnp.bfloat16)
    head_column = turned(jnp.broadcast_to(head_decay, (8, seq_len)))[:, 0:1]
    log_decay = head_column - decay_factor * sigmoid(turned(decay_input) + decay_offset)
    learn = turned(sigmoid(step_logits.astype(jnp.float32)))
    unit = key_vec * lax.rsqrt(jnp.sum(key_vec * key_vec, axis=1, keepdims=True) + key_eps)
    write = unit * learn
    keyed = key_vec * learn

    row = lax.broadcasted_iota(jnp.int32, (seq_len, seq_len), 0)
    col = lax.broadcasted_iota(jnp.int32, (seq_len, seq_len), 1)
    same = (row >> 5) == (col >> 5)
    upto = same & (col <= row)
    before = same & (col < row)

    log_top, log_rest = split_two(log_decay)
    log_low = (log_decay - log_top.astype(jnp.float32) - log_rest.astype(jnp.float32)).astype(jnp.bfloat16)
    summed = dot_f32(
        jnp.where(upto, 1.0, 0.0).astype(jnp.bfloat16),
        jnp.concatenate([log_top, log_rest, log_low], axis=1),
    )
    total = summed[:, :64] + summed[:, 64:128] + summed[:, 128:192]
    by_chunk = total.reshape(chunks, chunk_len, HEAD_CHANNELS)
    middle = jnp.broadcast_to(by_chunk[:, chunk_len // 2 - 1 : chunk_len // 2], by_chunk.shape).reshape(total.shape)
    last = by_chunk[:, chunk_len - 1 : chunk_len]
    ending = jnp.broadcast_to(last, by_chunk.shape).reshape(total.shape)
    prior = total - log_decay

    up_scale = jnp.exp(middle - total)
    scaled = jnp.concatenate([write * up_scale, keyed * up_scale], axis=0)
    gram = product_nt(-unit * jnp.exp(prior - middle), scaled)
    erase_write = jnp.where(before, gram[:, :seq_len], 0.0)
    erase_keyed = jnp.where(before, gram[:, seq_len:], 0.0)

    def below(width):
        return (
            ((row & (-2 * width)) == (col & (-2 * width)))
            & ((row & width) != 0)
            & ((col & width) == 0)
        )

    solved = jnp.where(row == col, 1.0, 0.0) + jnp.where(below(1), erase_write, 0.0)
    for width in (2, 4, 8, 16):
        solved = solved + product(solved, product(jnp.where(below(width), erase_write, 0.0), solved))

    def on_values(weights):
        top, low = split_two(weights)
        return dot_f32(
            jnp.concatenate([top, low], axis=1),
            jnp.concatenate([value_matrix, value_matrix], axis=0),
        )

    erased = product(
        solved, jnp.concatenate([-unit * jnp.exp(prior), on_values(erase_keyed)], axis=1)
    )
    tail_scale = jnp.exp(ending - total)
    wide_row = lax.broadcasted_iota(jnp.int32, (seq_len, chunks * 64), 0)
    wide_col = lax.broadcasted_iota(jnp.int32, (seq_len, chunks * 64), 1)
    in_block = (wide_row >> 5) == (wide_col >> 6)
    write_tail = jnp.where(in_block, jnp.concatenate([write * tail_scale] * chunks, axis=1), 0.0)
    keyed_tail = jnp.where(in_block, jnp.concatenate([keyed * tail_scale] * chunks, axis=1), 0.0)
    erased_t = jnp.transpose(erased)
    maps = product(erased_t, write_tail)
    keyed_top, keyed_low = split_two(keyed_tail)
    adds = maps[64:] + dot_f32(
        jnp.concatenate([value_t, value_t], axis=1),
        jnp.concatenate([keyed_top, keyed_low], axis=0),
    )
    small_row = lax.broadcasted_iota(jnp.int32, (64, 64), 0)
    small_col = lax.broadcasted_iota(jnp.int32, (64, 64), 1)
    eye = small_row == small_col

    def joined(early, late):
        moved = product(early, late[:64])
        return jnp.concatenate([moved[:64], moved[64:] + late[64:]], axis=0)

    steps = []
    for c in range(chunks):
        step_map = maps[:64, c * 64 : (c + 1) * 64] + jnp.where(eye, jnp.exp(last[c]), 0.0)
        steps.append(jnp.concatenate([step_map, adds[:, c * 64 : (c + 1) * 64]], axis=0))
    pairs = [joined(steps[2 * i], steps[2 * i + 1]) for i in range(4)]
    quads = [joined(pairs[0], pairs[1]), joined(pairs[2], pairs[3])]

    def outputs():
        gram_read = product_nt(read_vec * jnp.exp(total - middle), scaled)
        read_write = jnp.where(upto, gram_read[:, :seq_len], 0.0)
        read_keyed = jnp.where(upto, gram_read[:, seq_len:], 0.0)
        shown = product(read_write, erased)
        seen = read_vec * jnp.exp(total) + shown[:, :64]
        own = shown[:, 64:] + on_values(read_keyed)
        six = joined(quads[0], pairs[2])
        entering = (
            steps[0],
            pairs[0],
            joined(pairs[0], steps[2]),
            quads[0],
            joined(quads[0], steps[4]),
            six,
            joined(six, steps[6]),
        )
        through = [seen[:chunk_len]]
        local = [own[:chunk_len]]
        for c in range(1, chunks):
            part = slice(c * chunk_len, (c + 1) * chunk_len)
            viewed = product_nt(seen[part], entering[c - 1])
            through.append(viewed[:, :64])
            local.append(viewed[:, 64:] + own[part])
        return jnp.concatenate(through, axis=0), jnp.concatenate(local, axis=0)

    return joined(quads[0], quads[1]), outputs


MESH = pl.DeviceIdType.MESH
sub_rows = 16
subs = 4
half = 1024
width = 2048


def transfer(source, target, send, arrive, sp, tp):
    return pltpu.make_async_remote_copy(
        src_ref=source,
        dst_ref=target,
        send_sem=send,
        recv_sem=arrive,
        device_id=(sp, tp),
        device_id_type=MESH,
    )


def settle(block, sem):
    pltpu.make_async_copy(block, block, sem).wait()


def split_three(value):
    top, low = split_two(value)
    return top, low, (value - top.astype(jnp.float32) - low.astype(jnp.float32)).astype(jnp.bfloat16)


def ranks_of(first, second):
    count = first.shape[0]
    lane = lax.broadcasted_iota(jnp.int32, (count, 128), 1).astype(jnp.float32)
    hit_0 = jnp.where(lane == first, 1.0, 0.0)
    hit_1 = jnp.where(lane == second, 1.0, 0.0)
    row = lax.broadcasted_iota(jnp.int32, (count, count), 0)
    col = lax.broadcasted_iota(jnp.int32, (count, count), 1)
    same = (row >> 4) == (col >> 4)
    earlier = dot_f32(
        jnp.where(same & (col < row), 1.0, 0.0).astype(jnp.bfloat16),
        jnp.concatenate([hit_0, hit_1], axis=1).astype(jnp.bfloat16),
    )
    every = dot_f32(jnp.where(same, 1.0, 0.0).astype(jnp.bfloat16), hit_0.astype(jnp.bfloat16))
    rank_0 = jnp.sum(earlier[:, :128] * hit_0, axis=1, keepdims=True)
    rank_1 = jnp.sum((earlier[:, 128:] + every) * hit_1, axis=1, keepdims=True)
    return rank_0, rank_1


def fold_states(states):
    nodes = []
    for i in range(8):
        early, late = states[2 * i], states[2 * i + 1]
        stacked = jnp.concatenate([early[:, :64], early[:, 64:]], axis=0)
        moved = dot_f32(stacked, late[:, :64])
        nodes.append((moved[:64], moved[64:] + late[:, 64:].astype(jnp.float32)))
    while len(nodes) > 1:
        joined = []
        for i in range(0, len(nodes), 2):
            (early_map, early_state), (late_map, late_state) = nodes[i], nodes[i + 1]
            if i == 0:
                joined.append((None, product(early_state, late_map) + late_state))
            else:
                moved = product(jnp.concatenate([early_map, early_state], axis=0), late_map)
                joined.append((moved[:64], moved[64:] + late_state))
        nodes = joined
    return nodes[0][1]


def finish(mixer_out, head_norm_scale, head_gate_rows):
    average = jnp.mean(mixer_out, axis=1, keepdims=True)
    centred = mixer_out - average
    spread = jnp.mean(centred * centred, axis=1, keepdims=True)
    return centred * lax.rsqrt(spread + group_eps) * head_norm_scale * head_gate_rows


def layer_kernel(
    r_ref,
    k_ref,
    v_ref,
    d_ref,
    o_ref,
    h_ref,
    c_ref,
    g_ref,
    scale_ref,
    residual_ref,
    norm_ref,
    index_ref,
    score_ref,
    mix_hbm,
    gate_hbm,
    up_hbm,
    down_hbm,
    out_ref,
    mix_mat,
    gate_mat,
    up_mat,
    down_mat,
    gate_nat,
    up_nat,
    through_ref,
    local_ref,
    state_out,
    states,
    heads_out,
    heads_in,
    mixed_ref,
    table_ref,
    outgoing,
    incoming,
    codes,
    rows_all,
    gate_act,
    hidden_rows,
    mine_part,
    pair_out,
    pair_in,
    leave,
    back,
    sent_sum,
    pair_out_s,
    pair_in_s,
    leave_s,
    back_s,
    sent_sum_s,
    got_sum,
    weight_sem,
    state_send,
    state_recv,
    single_sem,
    spread_recv,
    ring_recv,
    twin_recv,
    pair_send,
    pair_recv,
    back_send,
    back_recv,
):
    sp, tp = lax.axis_index("sp"), lax.axis_index("tp")
    level, core = tp // 2, tp % 2
    twin = level * 2 + (1 - core)
    heads_send, heads_recv, spread_send, ring_send, twin_send, sum_send, sum_recv = (
        single_sem.at[k] for k in range(7)
    )

    loads = [
        pltpu.make_async_copy(source, target, weight_sem.at[k])
        for k, (source, target) in enumerate(
            (
                (mix_hbm, mix_mat),
                (gate_hbm.at[0], gate_mat),
                (up_hbm.at[0], up_mat),
                (down_hbm.at[0], down_mat),
            )
        )
    ]
    for load in loads:
        load.start()

    start_row = lax.broadcasted_iota(jnp.int32, (16, 64, 128), 1)
    start_col = lax.broadcasted_iota(jnp.int32, (16, 64, 128), 2)
    states[...] = jnp.where(start_row == start_col, 1.0, 0.0).astype(jnp.bfloat16)

    barrier = pltpu.get_barrier_semaphore()
    for j in range(1, 16):
        pl.semaphore_signal(barrier, inc=1, device_id=((sp + j) % 16, tp), device_id_type=MESH)
        pl.semaphore_signal(barrier, inc=1, device_id=(sp, (tp + j) % 16), device_id_type=MESH)

    final, outputs = mixer_local(
        r_ref[...], k_ref[...], v_ref[...], d_ref[...], o_ref[...], h_ref[...], c_ref[...]
    )
    state_out[...] = jnp.concatenate([final[:64], final[64:]], axis=1).astype(jnp.bfloat16)
    own_table = jnp.transpose(
        jnp.concatenate(
            [
                jnp.concatenate([index_ref[...].astype(jnp.float32), score_ref[...]], axis=0),
                jnp.zeros((4, 112), jnp.float32),
            ],
            axis=1,
        )
    )[:16]
    table_ref[...] = own_table

    pl.semaphore_wait(barrier, 30)

    def state_copy(j, source, target):
        return transfer(
            state_out, states.at[source], state_send.at[j], state_recv.at[source], target, tp
        )

    for j in range(1, 16):

        @pl.when(sp + j < 16)
        def _():
            state_copy(j, sp, sp + j).start()

    through_ref[...], local_ref[...] = outputs()

    own_table = table_ref[...]
    rank_0, rank_1 = ranks_of(own_table[:, 0:1], own_table[:, 1:2])
    first, second = own_table[:, 0:1] * 16.0 + rank_0, own_table[:, 1:2] * 16.0 + rank_1
    lane = lax.broadcasted_iota(jnp.int32, (16, 256), 1).astype(jnp.float32)
    spread = jnp.transpose(
        jnp.concatenate(
            [
                jnp.where((lane == first + 4.0 * q) | (lane == second + 4.0 * q), 1.0, 0.0)
                for q in range(4)
            ],
            axis=0,
        )
    ).astype(jnp.bfloat16)

    for j in range(1, 16):

        @pl.when(sp - j >= 0)
        def _():
            state_copy(j, sp - j, sp).wait_recv()

    entering = fold_states(states[...])
    attended = finish(
        local_ref[...] + product_nt(through_ref[...], entering), scale_ref[...], turned(g_ref[...])
    )
    score_parts = [
        part for k in (2, 3) for part in split_three(own_table[:, k : k + 1])
    ]
    notes = jnp.concatenate(
        [own_table[:, 0:2].astype(jnp.bfloat16)] + score_parts + [jnp.zeros((16, 56), jnp.bfloat16)],
        axis=1,
    ).astype(jnp.float32)
    notes = jnp.broadcast_to(
        jnp.concatenate([notes, notes], axis=1)[None], (16, 16, 128)
    )
    both = jnp.concatenate([attended, attended], axis=1).reshape(16, 16, 128)
    side_lane = lax.broadcasted_iota(jnp.int32, (16, 16, 128), 2) // 64
    heads_out[...] = jnp.where(side_lane == core, both, notes).astype(jnp.bfloat16)
    for j in range(1, 16):
        other = (tp + j) % 16
        transfer(
            heads_out.at[other], heads_in.at[tp], heads_send, heads_recv, sp, other
        ).start()
    heads_in[tp] = heads_out[tp]

    for load in loads:
        load.wait()

    settle(heads_in.at[pl.ds(0, 15)], heads_recv)
    low_lane = lax.broadcasted_iota(jnp.int32, (16, 128), 1) < 64
    tokens = jnp.concatenate(
        [
            jnp.where(
                low_lane,
                heads_in[2 * i].astype(jnp.float32),
                heads_in[2 * i + 1].astype(jnp.float32),
            ).astype(jnp.bfloat16)
            for i in range(8)
        ],
        axis=1,
    )
    mixed_f = (
        (residual_ref[...].astype(jnp.float32) + dot_f32(tokens, mix_mat[...]))
        .astype(jnp.bfloat16)
        .astype(jnp.float32)
    )
    mixed_ref[...] = mixed_f
    normed = (
        mixed_f
        * lax.rsqrt(jnp.mean(mixed_f * mixed_f, axis=1, keepdims=True) + norm_eps)
        * norm_ref[...]
    ).astype(jnp.bfloat16)
    stacked = jnp.concatenate([normed[:, q * 512 : (q + 1) * 512] for q in range(4)], axis=0)
    outgoing[...] = dot_f32(spread, stacked).astype(jnp.bfloat16).reshape(16, 16, 512)
    row_at, col_at = sp // 4, sp % 4

    def spread_copy(source, target, at):
        return transfer(
            outgoing.at[target], incoming.at[source], spread_send, spread_recv.at[at], target, tp
        )

    for i in range(4):
        for k in range(4):
            if i == 0 and k == 0:
                continue
            other = ((row_at + 4 - i) % 4) * 4 + (col_at + k) % 4
            spread_copy(sp, other, i).start()
    incoming[sp] = outgoing[sp]

    noted = heads_in[...].astype(jnp.float32)
    every = jnp.concatenate(
        [noted[t][:, (1 - t % 2) * 64 : (1 - t % 2) * 64 + 8] for t in range(16)], axis=0
    )
    score_0 = every[:, 2:3] + every[:, 3:4] + every[:, 4:5]
    score_1 = every[:, 5:6] + every[:, 6:7] + every[:, 7:8]
    rank_0, rank_1 = ranks_of(every[:, 0:1], every[:, 1:2])
    gap = score_1 - score_0
    wide_lane = lax.broadcasted_iota(jnp.int32, (256, 128), 1)
    kept = jnp.zeros((256, 128), jnp.float32)
    for at, column in enumerate(
        (
            every[:, 0:1] * 16.0 + rank_0,
            every[:, 1:2] * 16.0 + rank_1,
            1.0 / (1.0 + jnp.exp(gap)),
            1.0 / (1.0 + jnp.exp(-gap)),
            every[:, 0:1] * 8.0 + rank_0,
            every[:, 1:2] * 8.0 + rank_1,
        )
    ):
        kept = jnp.where(wide_lane == at, column, kept)
    codes[...] = kept.reshape(16, 16, 128)

    following = (((level + 1) % 8) * 2 + core, ((level + 7) % 8) * 2 + core)

    def block_at(distance, way):
        if way == 0:
            return (level + 8 - distance) % 8
        return (level + distance) % 8

    def turn(sub):
        return (row_at + sub) % 4

    def piece_of(index, sub):
        return rows_all.at[index, pl.ds(pl.multiple_of(turn(sub) * sub_rows, sub_rows), sub_rows)]

    def arrival(distance, sub, way):
        return (distance - 1) * subs + sub if distance < 4 else 3 * subs + sub % 2

    def travels(distance, sub, way):
        return distance < 4 or (sub < 2) == (way == 0)

    def ring(index, sub, distance, way):
        slot = arrival(distance, sub, way)
        return transfer(
            piece_of(index, sub),
            piece_of(index, sub),
            ring_send,
            ring_recv.at[way, slot],
            sp,
            following[way],
        )

    def twinned(index, sub, distance):
        return transfer(
            piece_of(index, sub), piece_of(index, sub), twin_send, twin_recv.at[distance], sp, twin
        )

    small_row = lax.broadcasted_iota(jnp.int32, (64, 64), 0)
    small_col = lax.broadcasted_iota(jnp.int32, (64, 64), 1)
    regroup = jnp.where(
        small_col == ((small_row >> 2) & 3) * 16 + (small_row >> 4) * 4 + (small_row & 3), 1.0, 0.0
    ).astype(jnp.bfloat16)
    for sub in range(subs):
        settle(incoming.at[pl.ds(0, 3 if sub == 0 else 4)], spread_recv.at[sub])
        regrouped = dot_f32(
            regroup, incoming[pl.ds(turn(sub) * 4, 4)].reshape(64, 512)
        ).astype(jnp.bfloat16)
        rows_all[tp, pl.ds(pl.multiple_of(turn(sub) * sub_rows, sub_rows), sub_rows)] = (
            jnp.concatenate([regrouped[q * 16 : (q + 1) * 16] for q in range(4)], axis=1)
        )
        for way in (0, 1):
            ring(tp, sub, 1, way).start()
        twinned(tp, sub, 0).start()

    def forward(distance, sub):
        for way in (0, 1):
            if not travels(distance, sub, way):
                continue
            index = block_at(distance, way) * 2 + core
            ring(index, sub, distance, way).wait_recv()
            if distance < 4 and travels(distance + 1, sub, way):
                ring(index, sub, distance + 1, way).start()
            twinned(index, sub, distance).start()

    def await_twin(distance):
        settle(rows_all.at[pl.ds(0, 1 if distance in (0, 4) else 2)], twin_recv.at[distance])

    def members(distance):
        low = block_at(distance, 0) * 2
        if distance in (0, 4):
            return (low, low + 1)
        high = block_at(distance, 1) * 2
        return (low, low + 1, high, high + 1)

    def buffers(distance):
        if distance in (0, 4):
            at = distance // 4
            return (
                pair_out_s.at[at],
                pair_in_s.at[at],
                leave_s.at[at],
                back_s.at[at],
                sent_sum_s.at[at],
            )
        at = distance - 1
        return pair_out.at[at], pair_in.at[at], leave.at[at], back.at[at], sent_sum.at[at]

    def order_of(parts):
        count = parts * 64
        row = lax.broadcasted_iota(jnp.int32, (count, count), 0)
        col = lax.broadcasted_iota(jnp.int32, (count, count), 1)
        source = ((row >> 2) & (parts - 1)) * 64 + (row // (4 * parts)) * 4 + (row & 3)
        return jnp.where(col == source, 1.0, 0.0).astype(jnp.bfloat16)

    reorder = {2: order_of(2), 4: order_of(4)}
    core_at = pl.multiple_of(core * half, half)
    twin_at = pl.multiple_of((1 - core) * half, half)
    across = (((1,), (1,)), ((), ()))

    gate_nat[...] = jnp.transpose(gate_mat[...])
    up_nat[...] = jnp.transpose(up_mat[...])

    def rows_in(distance):
        return jnp.concatenate([rows_all[index] for index in members(distance)], axis=0)

    def stage_gate(distance):
        count = 64 * len(members(distance))
        gate_act[:count] = dot_f32(rows_in(distance), gate_nat[...])

    def stage_up(distance):
        parts = len(members(distance))
        up_act = dot_f32(rows_in(distance), up_nat[...])
        gate = gate_act[: 64 * parts]
        hidden = (gate / (1.0 + jnp.exp(-gate)) * up_act).astype(jnp.bfloat16)
        hidden_rows[: 64 * parts] = dot_f32(reorder[parts], hidden).astype(jnp.bfloat16)

    def pair(distance):
        out, arrived = buffers(distance)[:2]
        return transfer(out, arrived, pair_send.at[distance], pair_recv.at[distance], sp, twin)

    def stage_other(distance):
        count = 64 * len(members(distance))
        buffers(distance)[0][...] = dot_f32(
            hidden_rows[:count], down_mat[:, pl.ds(twin_at, half)]
        ).astype(jnp.bfloat16)
        pair(distance).start()

    def stage_mine(distance):
        count = 64 * len(members(distance))
        mine_part[:count] = dot_f32(hidden_rows[:count], down_mat[:, pl.ds(core_at, half)])

    def back_copy(distance, source, target):
        _, _, out, arrived, _ = buffers(distance)
        return transfer(
            out.at[target],
            arrived.at[source],
            back_send.at[distance],
            back_recv.at[distance],
            target,
            tp,
        )

    def stage_return(distance):
        parts = len(members(distance))
        _, arrived, out, home, _ = buffers(distance)
        pair(distance).wait_recv()
        out[...] = (
            (mine_part[: 64 * parts] + arrived[...].astype(jnp.float32))
            .reshape(16, 4 * parts, half)
            .astype(jnp.bfloat16)
        )
        for j in range(1, 16):
            back_copy(distance, sp, (sp + j) % 16).start()
        home[sp] = out[sp]

    def stage_combine(distance):
        parts = len(members(distance))
        _, _, _, home, leaving = buffers(distance)
        settle(home.at[pl.ds(0, 15)], back_recv.at[distance])
        column = 0 if parts == 4 else 4
        columns = 64 * parts
        lanes = lax.broadcasted_iota(jnp.int32, (16, columns), 1).astype(jnp.float32)
        weights = []
        for place_in, index in enumerate(members(distance)):
            code = codes[index]
            first_at = code[:, column : column + 1] + 4.0 * place_in
            second_at = code[:, column + 1 : column + 2] + 4.0 * place_in
            weights.append(
                jnp.where(lanes == first_at, code[:, 2:3], 0.0)
                + jnp.where(lanes == second_at, code[:, 3:4], 0.0)
            )
        top, low = split_two(jnp.concatenate(weights, axis=0))
        returned = (
            home[...].astype(jnp.float32).reshape(columns, half).astype(jnp.bfloat16)
            if parts == 2
            else home[...].reshape(columns, half)
        )
        leaving[...] = (
            (dot_f32(top, returned) + dot_f32(low, returned)).astype(jnp.bfloat16).reshape(parts, 16, half)
        )

        def send(place_in, index):
            transfer(leaving.at[place_in], got_sum.at[tp], sum_send, sum_recv, sp, index).start()

        if distance == 0:
            send(1 - core, twin)
            got_sum[tp] = leaving[core]
        else:
            for place_in, index in enumerate(members(distance)):
                send(place_in, index)

    for distance in (0, 1, 2, 3):
        await_twin(distance)
        stage_gate(distance)
        forward(distance + 1, 0)
        stage_up(distance)
        forward(distance + 1, 1)
        stage_other(distance)
        forward(distance + 1, 2)
        stage_mine(distance)
        forward(distance + 1, 3)
        stage_return(distance)
        if distance > 0:
            stage_combine(distance - 1)
    await_twin(4)
    stage_gate(4)
    stage_up(4)
    stage_other(4)
    stage_mine(4)
    stage_return(4)
    stage_combine(3)
    stage_combine(4)

    settle(got_sum.at[pl.ds(0, 15)], sum_recv)
    for side in (0, 1):
        gathered = got_sum[side].astype(jnp.float32)
        for stage in range(1, 8):
            gathered = gathered + got_sum[2 * stage + side].astype(jnp.float32)
        cut = slice(side * half, (side + 1) * half)
        out_ref[:, cut] = mixed_ref[:, cut] + gathered
    settle(heads_out.at[pl.ds(0, 15)], heads_send)
    settle(outgoing.at[pl.ds(0, 15)], spread_send)
    settle(rows_all.at[pl.ds(0, 7)], ring_send)
    settle(rows_all.at[pl.ds(0, 8)], twin_send)
    settle(got_sum.at[pl.ds(0, 15)], sum_send)
    for distance in range(5):
        pair(distance).wait_send()
        settle(buffers(distance)[2].at[pl.ds(0, 15)], back_send.at[distance])
    for j in range(1, 16):

        @pl.when(sp + j < 16)
        def _():
            state_copy(j, sp, sp + j).wait_send()


def shards(
    receptance,
    key_matrix,
    value_matrix,
    decay_input_term,
    decay_channel_offset,
    head_log_decay,
    context_step_logits,
    head_gate_rows,
    head_norm_scale,
    mixer_output_weight,
    residual,
    expert_norm_scale,
    expert_index_table,
    expert_router_scores,
    expert_gate_weight,
    expert_up_weight,
    expert_down_weight,
):
    vmem = pl.BlockSpec(memory_space=pltpu.VMEM)
    hbm = pl.BlockSpec(memory_space=pl.ANY)
    dma = pltpu.SemaphoreType.DMA
    b16, f32 = jnp.bfloat16, jnp.float32
    total = pl.pallas_call(
        layer_kernel,
        out_shape=jax.ShapeDtypeStruct((16, width), f32),
        in_specs=[vmem] * 13 + [hbm] * 4,
        out_specs=vmem,
        scratch_shapes=[
            pltpu.VMEM((1024, width), b16),
            pltpu.VMEM((448, width), b16),
            pltpu.VMEM((448, width), b16),
            pltpu.VMEM((448, width), b16),
            pltpu.VMEM((width, 448), b16),
            pltpu.VMEM((width, 448), b16),
            pltpu.VMEM((seq_len, 64), f32),
            pltpu.VMEM((seq_len, 64), f32),
            pltpu.VMEM((64, 128), b16),
            pltpu.VMEM((16, 64, 128), b16),
            pltpu.VMEM((16, 16, 128), b16),
            pltpu.VMEM((16, 16, 128), b16),
            pltpu.VMEM((16, width), f32),
            pltpu.VMEM((16, 4), f32),
            pltpu.VMEM((16, 16, 512), b16),
            pltpu.VMEM((16, 16, 512), b16),
            pltpu.VMEM((16, 16, 128), f32),
            pltpu.VMEM((16, 64, width), b16),
            pltpu.VMEM((256, 448), f32),
            pltpu.VMEM((256, 448), b16),
            pltpu.VMEM((256, half), f32),
            pltpu.VMEM((3, 256, half), b16),
            pltpu.VMEM((3, 256, half), b16),
            pltpu.VMEM((3, 16, 16, half), b16),
            pltpu.VMEM((3, 16, 16, half), b16),
            pltpu.VMEM((3, 4, 16, half), b16),
            pltpu.VMEM((2, 128, half), b16),
            pltpu.VMEM((2, 128, half), b16),
            pltpu.VMEM((2, 16, 8, half), b16),
            pltpu.VMEM((2, 16, 8, half), b16),
            pltpu.VMEM((2, 2, 16, half), b16),
            pltpu.VMEM((16, 16, half), b16),
            dma((4,)),
            dma((16,)),
            dma((16,)),
            dma((7,)),
            dma((4,)),
            dma((2, 14)),
        ]
        + [dma((5,))] * 5,
        compiler_params=pltpu.CompilerParams(
            collective_id=1, has_side_effects=True, vmem_limit_bytes=56 * 1024 * 1024
        ),
    )(
        receptance.T,
        key_matrix.T,
        value_matrix.T,
        decay_input_term.T,
        decay_channel_offset.reshape(1, -1),
        head_log_decay.T,
        context_step_logits.T,
        head_gate_rows.T,
        head_norm_scale.reshape(1, -1),
        residual,
        expert_norm_scale.reshape(1, -1),
        expert_index_table.T,
        expert_router_scores.T,
        mixer_output_weight,
        jnp.swapaxes(expert_gate_weight, 1, 2),
        jnp.swapaxes(expert_up_weight, 1, 2),
        expert_down_weight,
    )
    return total.astype(b16)


def solution(mesh):
    return jax.shard_map(
        shards,
        mesh=mesh,
        in_specs=(
            P("sp", "tp"),
            P("sp", "tp"),
            P("sp", "tp"),
            P("sp", "tp"),
            P("tp"),
            P("sp", "tp"),
            P("sp", "tp"),
            P("sp", "tp"),
            P("tp"),
            P(),
            P(("sp", "tp"), None),
            P(),
            P(("sp", "tp"), None),
            P(("sp", "tp"), None),
            P("sp", None, "tp"),
            P("sp", None, "tp"),
            P("sp", "tp", None),
        ),
        out_specs=P(("sp", "tp"), None),
        check_vma=False,
    )
```

```python
import jax
import jax.numpy as jnp
from jax import lax
from jax.experimental import pallas as pl
from jax.experimental.pallas import tpu as pltpu
from jax.sharding import PartitionSpec as P

HEAD_CHANNELS = 64

decay_factor = 0.6065306597126334
group_eps = 0.00064
norm_eps = 1e-06
key_eps = 1e-06
seq_len = 256
chunk_len = 32
chunks = seq_len // chunk_len


def split_two(value):
    top = value.astype(jnp.bfloat16)
    return top, (value - top.astype(jnp.float32)).astype(jnp.bfloat16)


def dot_f32(left, right, dims=(((1,), (0,)), ((), ()))):
    return lax.dot_general(left, right, dims, preferred_element_type=jnp.float32)


def product(left, right):
    left_top, left_low = split_two(left)
    right_top, right_low = split_two(right)
    return dot_f32(
        jnp.concatenate([left_top, left_top, left_low], axis=1),
        jnp.concatenate([right_top, right_low, right_top], axis=0),
    )


def product_nt(left, right):
    left_top, left_low = split_two(left)
    right_top, right_low = split_two(right)
    return dot_f32(
        jnp.concatenate([left_top, left_top, left_low], axis=1),
        jnp.concatenate([right_top, right_low, right_top], axis=1),
        (((1,), (1,)), ((), ())),
    )


def sigmoid(value):
    return 1.0 / (1.0 + jnp.exp(-value))


def turned(value):
    return jnp.transpose(value.astype(jnp.float32))


def mixer_local(receptance, key_matrix, value_t, decay_input, decay_offset, head_decay, step_logits):
    read_vec, key_vec = turned(receptance), turned(key_matrix)
    value_matrix = turned(value_t).astype(jnp.bfloat16)
    head_column = turned(jnp.broadcast_to(head_decay, (8, seq_len)))[:, 0:1]
    log_decay = head_column - decay_factor * sigmoid(turned(decay_input) + decay_offset)
    learn = turned(sigmoid(step_logits.astype(jnp.float32)))
    unit = key_vec * lax.rsqrt(jnp.sum(key_vec * key_vec, axis=1, keepdims=True) + key_eps)
    write = unit * learn
    keyed = key_vec * learn

    row = lax.broadcasted_iota(jnp.int32, (seq_len, seq_len), 0)
    col = lax.broadcasted_iota(jnp.int32, (seq_len, seq_len), 1)
    same = (row >> 5) == (col >> 5)
    upto = same & (col <= row)
    before = same & (col < row)

    log_top, log_rest = split_two(log_decay)
    log_low = (log_decay - log_top.astype(jnp.float32) - log_rest.astype(jnp.float32)).astype(jnp.bfloat16)
    summed = dot_f32(
        jnp.where(upto, 1.0, 0.0).astype(jnp.bfloat16),
        jnp.concatenate([log_top, log_rest, log_low], axis=1),
    )
    total = summed[:, :64] + summed[:, 64:128] + summed[:, 128:192]
    by_chunk = total.reshape(chunks, chunk_len, HEAD_CHANNELS)
    middle = jnp.broadcast_to(by_chunk[:, chunk_len // 2 - 1 : chunk_len // 2], by_chunk.shape).reshape(total.shape)
    last = by_chunk[:, chunk_len - 1 : chunk_len]
    ending = jnp.broadcast_to(last, by_chunk.shape).reshape(total.shape)
    prior = total - log_decay

    up_scale = jnp.exp(middle - total)
    scaled = jnp.concatenate([write * up_scale, keyed * up_scale], axis=0)
    gram = product_nt(-unit * jnp.exp(prior - middle), scaled)
    erase_write = jnp.where(before, gram[:, :seq_len], 0.0)
    erase_keyed = jnp.where(before, gram[:, seq_len:], 0.0)

    def below(width):
        return (
            ((row & (-2 * width)) == (col & (-2 * width)))
            & ((row & width) != 0)
            & ((col & width) == 0)
        )

    solved = jnp.where(row == col, 1.0, 0.0) + jnp.where(below(1), erase_write, 0.0)
    for width in (2, 4, 8, 16):
        solved = solved + product(solved, product(jnp.where(below(width), erase_write, 0.0), solved))

    def on_values(weights):
        top, low = split_two(weights)
        return dot_f32(
            jnp.concatenate([top, low], axis=1),
            jnp.concatenate([value_matrix, value_matrix], axis=0),
        )

    erased = product(
        solved, jnp.concatenate([-unit * jnp.exp(prior), on_values(erase_keyed)], axis=1)
    )
    tail_scale = jnp.exp(ending - total)
    wide_row = lax.broadcasted_iota(jnp.int32, (seq_len, chunks * 64), 0)
    wide_col = lax.broadcasted_iota(jnp.int32, (seq_len, chunks * 64), 1)
    in_block = (wide_row >> 5) == (wide_col >> 6)
    write_tail = jnp.where(in_block, jnp.concatenate([write * tail_scale] * chunks, axis=1), 0.0)
    keyed_tail = jnp.where(in_block, jnp.concatenate([keyed * tail_scale] * chunks, axis=1), 0.0)
    erased_t = jnp.transpose(erased)
    maps = product(erased_t, write_tail)
    keyed_top, keyed_low = split_two(keyed_tail)
    adds = maps[64:] + dot_f32(
        jnp.concatenate([value_t, value_t], axis=1),
        jnp.concatenate([keyed_top, keyed_low], axis=0),
    )
    small_row = lax.broadcasted_iota(jnp.int32, (64, 64), 0)
    small_col = lax.broadcasted_iota(jnp.int32, (64, 64), 1)
    eye = small_row == small_col

    def joined(early, late):
        moved = product(early, late[:64])
        return jnp.concatenate([moved[:64], moved[64:] + late[64:]], axis=0)

    steps = []
    for c in range(chunks):
        step_map = maps[:64, c * 64 : (c + 1) * 64] + jnp.where(eye, jnp.exp(last[c]), 0.0)
        steps.append(jnp.concatenate([step_map, adds[:, c * 64 : (c + 1) * 64]], axis=0))
    pairs = [joined(steps[2 * i], steps[2 * i + 1]) for i in range(4)]
    quads = [joined(pairs[0], pairs[1]), joined(pairs[2], pairs[3])]

    def outputs():
        gram_read = product_nt(read_vec * jnp.exp(total - middle), scaled)
        read_write = jnp.where(upto, gram_read[:, :seq_len], 0.0)
        read_keyed = jnp.where(upto, gram_read[:, seq_len:], 0.0)
        shown = product(read_write, erased)
        seen = read_vec * jnp.exp(total) + shown[:, :64]
        own = shown[:, 64:] + on_values(read_keyed)
        six = joined(quads[0], pairs[2])
        entering = (
            steps[0],
            pairs[0],
            joined(pairs[0], steps[2]),
            quads[0],
            joined(quads[0], steps[4]),
            six,
            joined(six, steps[6]),
        )
        through = [seen[:chunk_len]]
        local = [own[:chunk_len]]
        for c in range(1, chunks):
            part = slice(c * chunk_len, (c + 1) * chunk_len)
            viewed = product_nt(seen[part], entering[c - 1])
            through.append(viewed[:, :64])
            local.append(viewed[:, 64:] + own[part])
        return jnp.concatenate(through, axis=0), jnp.concatenate(local, axis=0)

    return joined(quads[0], quads[1]), outputs


MESH = pl.DeviceIdType.MESH
sub_rows = 16
subs = 4
half = 1024
width = 2048


def transfer(source, target, send, arrive, sp, tp):
    return pltpu.make_async_remote_copy(
        src_ref=source,
        dst_ref=target,
        send_sem=send,
        recv_sem=arrive,
        device_id=(sp, tp),
        device_id_type=MESH,
    )


def settle(block, sem):
    pltpu.make_async_copy(block, block, sem).wait()


def split_three(value):
    top, low = split_two(value)
    return top, low, (value - top.astype(jnp.float32) - low.astype(jnp.float32)).astype(jnp.bfloat16)


def ranks_of(first, second):
    count = first.shape[0]
    lane = lax.broadcasted_iota(jnp.int32, (count, 128), 1).astype(jnp.float32)
    hit_0 = jnp.where(lane == first, 1.0, 0.0)
    hit_1 = jnp.where(lane == second, 1.0, 0.0)
    row = lax.broadcasted_iota(jnp.int32, (count, count), 0)
    col = lax.broadcasted_iota(jnp.int32, (count, count), 1)
    same = (row >> 4) == (col >> 4)
    earlier = dot_f32(
        jnp.where(same & (col < row), 1.0, 0.0).astype(jnp.bfloat16),
        jnp.concatenate([hit_0, hit_1], axis=1).astype(jnp.bfloat16),
    )
    every = dot_f32(jnp.where(same, 1.0, 0.0).astype(jnp.bfloat16), hit_0.astype(jnp.bfloat16))
    rank_0 = jnp.sum(earlier[:, :128] * hit_0, axis=1, keepdims=True)
    rank_1 = jnp.sum((earlier[:, 128:] + every) * hit_1, axis=1, keepdims=True)
    return rank_0, rank_1


def fold_states(states):
    nodes = []
    for i in range(8):
        early, late = states[2 * i], states[2 * i + 1]
        stacked = jnp.concatenate([early[:, :64], early[:, 64:]], axis=0)
        moved = dot_f32(stacked, late[:, :64])
        nodes.append((moved[:64], moved[64:] + late[:, 64:].astype(jnp.float32)))
    while len(nodes) > 1:
        joined = []
        for i in range(0, len(nodes), 2):
            (early_map, early_state), (late_map, late_state) = nodes[i], nodes[i + 1]
            if i == 0:
                joined.append((None, product(early_state, late_map) + late_state))
            else:
                moved = product(jnp.concatenate([early_map, early_state], axis=0), late_map)
                joined.append((moved[:64], moved[64:] + late_state))
        nodes = joined
    return nodes[0][1]


def finish(mixer_out, head_norm_scale, head_gate_rows):
    average = jnp.mean(mixer_out, axis=1, keepdims=True)
    centred = mixer_out - average
    spread = jnp.mean(centred * centred, axis=1, keepdims=True)
    return centred * lax.rsqrt(spread + group_eps) * head_norm_scale * head_gate_rows


def layer_kernel(
    r_ref,
    k_ref,
    v_ref,
    d_ref,
    o_ref,
    h_ref,
    c_ref,
    g_ref,
    scale_ref,
    residual_ref,
    norm_ref,
    index_ref,
    score_ref,
    mix_hbm,
    gate_hbm,
    up_hbm,
    down_hbm,
    out_ref,
    mix_mat,
    gate_mat,
    up_mat,
    down_mat,
    gate_nat,
    up_nat,
    through_ref,
    local_ref,
    state_out,
    states,
    heads_out,
    heads_in,
    mixed_ref,
    table_ref,
    outgoing,
    incoming,
    raw_out,
    raw_in,
    far_out,
    far_in,
    codes,
    rows_all,
    gate_act,
    hidden_rows,
    mine_part,
    pair_out,
    pair_in,
    leave,
    back,
    sent_sum,
    pair_out_s,
    pair_in_s,
    leave_s,
    back_s,
    sent_sum_s,
    got_sum,
    weight_sem,
    state_send,
    state_recv,
    single_sem,
    spread_recv,
    ring_recv,
    twin_recv,
    pair_send,
    pair_recv,
    back_send,
    back_recv,
):
    sp, tp = lax.axis_index("sp"), lax.axis_index("tp")
    level, core = tp // 2, tp % 2
    twin = level * 2 + (1 - core)
    opposite = (tp + 8) % 16
    (
        heads_send,
        heads_recv,
        spread_send,
        ring_send,
        twin_send,
        sum_send,
        sum_recv,
        raw_send,
        raw_recv,
        far_send,
        far_recv,
    ) = (single_sem.at[k] for k in range(11))

    loads = [
        pltpu.make_async_copy(source, target, weight_sem.at[k])
        for k, (source, target) in enumerate(
            (
                (mix_hbm, mix_mat),
                (gate_hbm.at[0], gate_mat),
                (up_hbm.at[0], up_mat),
                (down_hbm.at[0], down_mat),
            )
        )
    ]
    for load in loads:
        load.start()

    start_row = lax.broadcasted_iota(jnp.int32, (16, 64, 128), 1)
    start_col = lax.broadcasted_iota(jnp.int32, (16, 64, 128), 2)
    states[...] = jnp.where(start_row == start_col, 1.0, 0.0).astype(jnp.bfloat16)

    barrier = pltpu.get_barrier_semaphore()
    for j in range(1, 16):
        pl.semaphore_signal(barrier, inc=1, device_id=((sp + j) % 16, tp), device_id_type=MESH)
        pl.semaphore_signal(barrier, inc=1, device_id=(sp, (tp + j) % 16), device_id_type=MESH)

    final, outputs = mixer_local(
        r_ref[...], k_ref[...], v_ref[...], d_ref[...], o_ref[...], h_ref[...], c_ref[...]
    )
    state_out[...] = jnp.concatenate([final[:64], final[64:]], axis=1).astype(jnp.bfloat16)
    own_table = jnp.transpose(
        jnp.concatenate(
            [
                jnp.concatenate([index_ref[...].astype(jnp.float32), score_ref[...]], axis=0),
                jnp.zeros((4, 112), jnp.float32),
            ],
            axis=1,
        )
    )[:16]
    table_ref[...] = own_table

    pl.semaphore_wait(barrier, 30)

    def state_copy(j, source, target):
        return transfer(
            state_out, states.at[source], state_send.at[j], state_recv.at[source], target, tp
        )

    for j in range(1, 16):

        @pl.when(sp + j < 16)
        def _():
            state_copy(j, sp, sp + j).start()

    through_ref[...], local_ref[...] = outputs()

    own_table = table_ref[...]
    rank_0, rank_1 = ranks_of(own_table[:, 0:1], own_table[:, 1:2])

    def spread_of(first, second):
        lane = lax.broadcasted_iota(jnp.int32, (16, 256), 1).astype(jnp.float32)
        return jnp.transpose(
            jnp.concatenate(
                [
                    jnp.where((lane == first + 4.0 * q) | (lane == second + 4.0 * q), 1.0, 0.0)
                    for q in range(4)
                ],
                axis=0,
            )
        ).astype(jnp.bfloat16)

    def spread_rows(spread, rows):
        stacked = jnp.concatenate([rows[:, q * 512 : (q + 1) * 512] for q in range(4)], axis=0)
        return dot_f32(spread, stacked).astype(jnp.bfloat16).reshape(16, 16, 512)

    spread = spread_of(own_table[:, 0:1] * 16.0 + rank_0, own_table[:, 1:2] * 16.0 + rank_1)

    for j in range(1, 16):

        @pl.when(sp - j >= 0)
        def _():
            state_copy(j, sp - j, sp).wait_recv()

    entering = fold_states(states[...])
    attended = finish(
        local_ref[...] + product_nt(through_ref[...], entering), scale_ref[...], turned(g_ref[...])
    )
    score_parts = [
        part for k in (2, 3) for part in split_three(own_table[:, k : k + 1])
    ]
    notes = jnp.concatenate(
        [own_table[:, 0:2].astype(jnp.bfloat16)] + score_parts + [jnp.zeros((16, 56), jnp.bfloat16)],
        axis=1,
    ).astype(jnp.float32)
    notes = jnp.broadcast_to(
        jnp.concatenate([notes, notes], axis=1)[None], (16, 16, 128)
    )
    both = jnp.concatenate([attended, attended], axis=1).reshape(16, 16, 128)
    side_lane = lax.broadcasted_iota(jnp.int32, (16, 16, 128), 2) // 64
    heads_out[...] = jnp.where(side_lane == core, both, notes).astype(jnp.bfloat16)
    for j in range(1, 16):
        other = (tp + j) % 16
        transfer(
            heads_out.at[other], heads_in.at[tp], heads_send, heads_recv, sp, other
        ).start()
    heads_in[tp] = heads_out[tp]

    for load in loads:
        load.wait()
    gate_nat[...] = jnp.transpose(gate_mat[...])

    settle(heads_in.at[pl.ds(0, 15)], heads_recv)
    low_lane = lax.broadcasted_iota(jnp.int32, (16, 128), 1) < 64
    tokens = jnp.concatenate(
        [
            jnp.where(
                low_lane,
                heads_in[2 * i].astype(jnp.float32),
                heads_in[2 * i + 1].astype(jnp.float32),
            ).astype(jnp.bfloat16)
            for i in range(8)
        ],
        axis=1,
    )
    mixed_f = (
        (residual_ref[...].astype(jnp.float32) + dot_f32(tokens, mix_mat[...]))
        .astype(jnp.bfloat16)
        .astype(jnp.float32)
    )
    mixed_ref[...] = mixed_f
    normed = (
        mixed_f
        * lax.rsqrt(jnp.mean(mixed_f * mixed_f, axis=1, keepdims=True) + norm_eps)
        * norm_ref[...]
    ).astype(jnp.bfloat16)
    raw_out[...] = normed
    raw_copy = transfer(raw_out, raw_in, raw_send, raw_recv, sp, opposite)
    raw_copy.start()
    outgoing[...] = spread_rows(spread, normed)
    row_at, col_at = sp // 4, sp % 4

    def spread_copy(source, target, at):
        return transfer(
            outgoing.at[target], incoming.at[source], spread_send, spread_recv.at[at], target, tp
        )

    for i in range(4):
        for k in range(4):
            if i == 0 and k == 0:
                continue
            other = ((row_at + 4 - i) % 4) * 4 + (col_at + k) % 4
            spread_copy(sp, other, i).start()
    incoming[sp] = outgoing[sp]

    noted = heads_in[...].astype(jnp.float32)
    every = jnp.concatenate(
        [noted[t][:, (1 - t % 2) * 64 : (1 - t % 2) * 64 + 8] for t in range(16)], axis=0
    )
    score_0 = every[:, 2:3] + every[:, 3:4] + every[:, 4:5]
    score_1 = every[:, 5:6] + every[:, 6:7] + every[:, 7:8]
    rank_0, rank_1 = ranks_of(every[:, 0:1], every[:, 1:2])
    gap = score_1 - score_0
    wide_lane = lax.broadcasted_iota(jnp.int32, (256, 128), 1)
    kept = jnp.zeros((256, 128), jnp.float32)
    for at, column in enumerate(
        (
            every[:, 0:1] * 16.0 + rank_0,
            every[:, 1:2] * 16.0 + rank_1,
            1.0 / (1.0 + jnp.exp(gap)),
            1.0 / (1.0 + jnp.exp(-gap)),
            every[:, 0:1] * 8.0 + rank_0,
            every[:, 1:2] * 8.0 + rank_1,
        )
    ):
        kept = jnp.where(wide_lane == at, column, kept)
    codes[...] = kept.reshape(16, 16, 128)
    up_nat[...] = jnp.transpose(up_mat[...])

    following = (((level + 1) % 8) * 2 + core, ((level + 7) % 8) * 2 + core)

    def block_at(distance, way):
        if way == 0:
            return (level + 8 - distance) % 8
        return (level + distance) % 8

    def turn(sub):
        return (row_at + sub) % 4

    def piece_of(index, sub):
        return rows_all.at[index, pl.ds(pl.multiple_of(turn(sub) * sub_rows, sub_rows), sub_rows)]

    def arrival(distance, sub):
        return (distance - 1) * subs + sub

    def ring(index, sub, distance, way):
        slot = arrival(distance, sub)
        return transfer(
            piece_of(index, sub),
            piece_of(index, sub),
            ring_send,
            ring_recv.at[way, slot],
            sp,
            following[way],
        )

    def twinned(index, sub, piece):
        return transfer(
            piece_of(index, sub), piece_of(index, sub), twin_send, twin_recv.at[piece], sp, twin
        )

    small_row = lax.broadcasted_iota(jnp.int32, (64, 64), 0)
    small_col = lax.broadcasted_iota(jnp.int32, (64, 64), 1)
    regroup = jnp.where(
        small_col == ((small_row >> 2) & 3) * 16 + (small_row >> 4) * 4 + (small_row & 3), 1.0, 0.0
    ).astype(jnp.bfloat16)
    for sub in range(subs):
        settle(incoming.at[pl.ds(0, 3 if sub == 0 else 4)], spread_recv.at[sub])
        regrouped = dot_f32(
            regroup, incoming[pl.ds(turn(sub) * 4, 4)].reshape(64, 512)
        ).astype(jnp.bfloat16)
        rows_all[tp, pl.ds(pl.multiple_of(turn(sub) * sub_rows, sub_rows), sub_rows)] = (
            jnp.concatenate([regrouped[q * 16 : (q + 1) * 16] for q in range(4)], axis=1)
        )
        for way in (0, 1):
            ring(tp, sub, 1, way).start()
        twinned(tp, sub, 0).start()

    raw_copy.wait_recv()
    far_codes = codes[opposite]
    far_out[...] = spread_rows(spread_of(far_codes[:, 0:1], far_codes[:, 1:2]), raw_in[...])
    for j in range(1, 16):
        other = (sp + j) % 16
        transfer(far_out.at[other], far_in.at[sp], far_send, far_recv, other, tp).start()
    far_in[sp] = far_out[sp]

    def far_arrives():
        settle(far_in.at[pl.ds(0, 15)], far_recv)
        for sub in range(subs):
            regrouped = dot_f32(
                regroup, far_in[sub * 4 : (sub + 1) * 4].reshape(64, 512)
            ).astype(jnp.bfloat16)
            rows_all[opposite, sub * sub_rows : (sub + 1) * sub_rows] = jnp.concatenate(
                [regrouped[q * 16 : (q + 1) * 16] for q in range(4)], axis=1
            )
        transfer(
            rows_all.at[opposite], rows_all.at[opposite], twin_send, twin_recv.at[4], sp, twin
        ).start()

    def forward(distance, sub):
        for way in (0, 1):
            index = block_at(distance, way) * 2 + core
            ring(index, sub, distance, way).wait_recv()
            if distance < 3:
                ring(index, sub, distance + 1, way).start()
            twinned(index, sub, 5 if distance == 3 and way == 1 else distance).start()

    def await_twin(distance):
        settle(rows_all.at[pl.ds(0, 2 if distance in (1, 2) else 1)], twin_recv.at[distance])

    def members(distance):
        low = block_at(3, 1) * 2 if distance == 5 else block_at(distance, 0) * 2
        if distance not in (1, 2):
            return (low, low + 1)
        high = block_at(distance, 1) * 2
        return (low, low + 1, high, high + 1)

    def buffers(distance):
        if distance not in (1, 2):
            at = (0, None, None, 2, 1, 3)[distance]
            return (
                pair_out_s.at[at],
                pair_in_s.at[at],
                leave_s.at[at],
                back_s.at[at],
                sent_sum_s.at[at],
            )
        at = distance - 1
        return pair_out.at[at], pair_in.at[at], leave.at[at], back.at[at], sent_sum.at[at]

    def order_of(parts):
        count = parts * 64
        row = lax.broadcasted_iota(jnp.int32, (count, count), 0)
        col = lax.broadcasted_iota(jnp.int32, (count, count), 1)
        source = ((row >> 2) & (parts - 1)) * 64 + (row // (4 * parts)) * 4 + (row & 3)
        return jnp.where(col == source, 1.0, 0.0).astype(jnp.bfloat16)

    reorder = {2: order_of(2), 4: order_of(4)}
    core_at = pl.multiple_of(core * half, half)
    twin_at = pl.multiple_of((1 - core) * half, half)
    across = (((1,), (1,)), ((), ()))

    def rows_in(distance):
        return jnp.concatenate([rows_all[index] for index in members(distance)], axis=0)

    def stage_gate(distance):
        count = 64 * len(members(distance))
        gate_act[:count] = dot_f32(rows_in(distance), gate_nat[...])

    def stage_up(distance):
        parts = len(members(distance))
        up_act = dot_f32(rows_in(distance), up_nat[...])
        gate = gate_act[: 64 * parts]
        hidden = (gate / (1.0 + jnp.exp(-gate)) * up_act).astype(jnp.bfloat16)
        hidden_rows[: 64 * parts] = dot_f32(reorder[parts], hidden).astype(jnp.bfloat16)

    def pair(distance):
        out, arrived = buffers(distance)[:2]
        return transfer(out, arrived, pair_send.at[distance], pair_recv.at[distance], sp, twin)

    def stage_other(distance):
        count = 64 * len(members(distance))
        buffers(distance)[0][...] = dot_f32(
            hidden_rows[:count], down_mat[:, pl.ds(twin_at, half)]
        ).astype(jnp.bfloat16)
        pair(distance).start()

    def stage_mine(distance):
        count = 64 * len(members(distance))
        mine_part[:count] = dot_f32(hidden_rows[:count], down_mat[:, pl.ds(core_at, half)])

    def back_copy(distance, source, target):
        _, _, out, arrived, _ = buffers(distance)
        return transfer(
            out.at[target],
            arrived.at[source],
            back_send.at[distance],
            back_recv.at[distance],
            target,
            tp,
        )

    def stage_return(distance):
        parts = len(members(distance))
        _, arrived, out, home, _ = buffers(distance)
        pair(distance).wait_recv()
        out[...] = (
            (mine_part[: 64 * parts] + arrived[...].astype(jnp.float32))
            .reshape(16, 4 * parts, half)
            .astype(jnp.bfloat16)
        )
        for j in range(1, 16):
            back_copy(distance, sp, (sp + j) % 16).start()
        home[sp] = out[sp]

    def stage_combine(distance):
        parts = len(members(distance))
        _, _, _, home, leaving = buffers(distance)
        settle(home.at[pl.ds(0, 15)], back_recv.at[distance])
        column = 0 if parts == 4 else 4
        columns = 64 * parts
        lanes = lax.broadcasted_iota(jnp.int32, (16, columns), 1).astype(jnp.float32)
        weights = []
        for place_in, index in enumerate(members(distance)):
            code = codes[index]
            first_at = code[:, column : column + 1] + 4.0 * place_in
            second_at = code[:, column + 1 : column + 2] + 4.0 * place_in
            weights.append(
                jnp.where(lanes == first_at, code[:, 2:3], 0.0)
                + jnp.where(lanes == second_at, code[:, 3:4], 0.0)
            )
        top, low = split_two(jnp.concatenate(weights, axis=0))
        returned = (
            home[...].astype(jnp.float32).reshape(columns, half).astype(jnp.bfloat16)
            if parts == 2
            else home[...].reshape(columns, half)
        )
        leaving[...] = (
            (dot_f32(top, returned) + dot_f32(low, returned)).astype(jnp.bfloat16).reshape(parts, 16, half)
        )

        def send(place_in, index):
            transfer(leaving.at[place_in], got_sum.at[tp], sum_send, sum_recv, sp, index).start()

        if distance == 0:
            send(1 - core, twin)
            got_sum[tp] = leaving[core]
        else:
            for place_in, index in enumerate(members(distance)):
                send(place_in, index)

    def stages_up(distance):
        await_twin(distance)
        stage_gate(distance)
        stage_up(distance)

    def stages_down(distance):
        stage_other(distance)
        stage_mine(distance)

    stages_up(0)
    forward(1, 0)
    stages_down(0)
    forward(1, 1)
    stage_return(0)
    forward(1, 2)
    forward(1, 3)
    stages_up(1)
    forward(2, 0)
    stages_down(1)
    far_arrives()
    forward(2, 1)
    stage_return(1)
    forward(2, 2)
    stages_up(4)
    stages_down(4)
    forward(2, 3)
    stage_return(4)
    stages_up(2)
    forward(3, 0)
    stages_down(2)
    forward(3, 1)
    stage_return(2)
    forward(3, 2)
    stage_combine(0)
    forward(3, 3)
    stages_up(3)
    stages_down(3)
    stages_up(5)
    stage_return(3)
    stages_down(5)
    stage_return(5)
    stage_combine(1)
    stage_combine(4)
    stage_combine(2)
    stage_combine(3)
    stage_combine(5)

    settle(got_sum.at[pl.ds(0, 15)], sum_recv)
    for side in (0, 1):
        gathered = got_sum[side].astype(jnp.float32)
        for stage in range(1, 8):
            gathered = gathered + got_sum[2 * stage + side].astype(jnp.float32)
        cut = slice(side * half, (side + 1) * half)
        out_ref[:, cut] = mixed_ref[:, cut] + gathered
    settle(heads_out.at[pl.ds(0, 15)], heads_send)
    settle(outgoing.at[pl.ds(0, 15)], spread_send)
    settle(rows_all.at[pl.ds(0, 6)], ring_send)
    settle(raw_out, raw_send)
    settle(far_out.at[pl.ds(0, 15)], far_send)
    settle(rows_all.at[pl.ds(0, 8)], twin_send)
    settle(got_sum.at[pl.ds(0, 15)], sum_send)
    for distance in range(6):
        pair(distance).wait_send()
        settle(buffers(distance)[2].at[pl.ds(0, 15)], back_send.at[distance])
    for j in range(1, 16):

        @pl.when(sp + j < 16)
        def _():
            state_copy(j, sp, sp + j).wait_send()


def shards(
    receptance,
    key_matrix,
    value_matrix,
    decay_input_term,
    decay_channel_offset,
    head_log_decay,
    context_step_logits,
    head_gate_rows,
    head_norm_scale,
    mixer_output_weight,
    residual,
    expert_norm_scale,
    expert_index_table,
    expert_router_scores,
    expert_gate_weight,
    expert_up_weight,
    expert_down_weight,
):
    vmem = pl.BlockSpec(memory_space=pltpu.VMEM)
    hbm = pl.BlockSpec(memory_space=pl.ANY)
    dma = pltpu.SemaphoreType.DMA
    b16, f32 = jnp.bfloat16, jnp.float32
    total = pl.pallas_call(
        layer_kernel,
        out_shape=jax.ShapeDtypeStruct((16, width), f32),
        in_specs=[vmem] * 13 + [hbm] * 4,
        out_specs=vmem,
        scratch_shapes=[
            pltpu.VMEM((1024, width), b16),
            pltpu.VMEM((448, width), b16),
            pltpu.VMEM((448, width), b16),
            pltpu.VMEM((448, width), b16),
            pltpu.VMEM((width, 448), b16),
            pltpu.VMEM((width, 448), b16),
            pltpu.VMEM((seq_len, 64), f32),
            pltpu.VMEM((seq_len, 64), f32),
            pltpu.VMEM((64, 128), b16),
            pltpu.VMEM((16, 64, 128), b16),
            pltpu.VMEM((16, 16, 128), b16),
            pltpu.VMEM((16, 16, 128), b16),
            pltpu.VMEM((16, width), f32),
            pltpu.VMEM((16, 4), f32),
            pltpu.VMEM((16, 16, 512), b16),
            pltpu.VMEM((16, 16, 512), b16),
            pltpu.VMEM((16, width), b16),
            pltpu.VMEM((16, width), b16),
            pltpu.VMEM((16, 16, 512), b16),
            pltpu.VMEM((16, 16, 512), b16),
            pltpu.VMEM((16, 16, 128), f32),
            pltpu.VMEM((16, 64, width), b16),
            pltpu.VMEM((256, 448), f32),
            pltpu.VMEM((256, 448), b16),
            pltpu.VMEM((256, half), f32),
            pltpu.VMEM((2, 256, half), b16),
            pltpu.VMEM((2, 256, half), b16),
            pltpu.VMEM((2, 16, 16, half), b16),
            pltpu.VMEM((2, 16, 16, half), b16),
            pltpu.VMEM((2, 4, 16, half), b16),
            pltpu.VMEM((4, 128, half), b16),
            pltpu.VMEM((4, 128, half), b16),
            pltpu.VMEM((4, 16, 8, half), b16),
            pltpu.VMEM((4, 16, 8, half), b16),
            pltpu.VMEM((4, 2, 16, half), b16),
            pltpu.VMEM((16, 16, half), b16),
            dma((4,)),
            dma((16,)),
            dma((16,)),
            dma((11,)),
            dma((4,)),
            dma((2, 12)),
        ]
        + [dma((6,))] * 5,
        compiler_params=pltpu.CompilerParams(
            collective_id=1, has_side_effects=True, vmem_limit_bytes=56 * 1024 * 1024
        ),
    )(
        receptance.T,
        key_matrix.T,
        value_matrix.T,
        decay_input_term.T,
        decay_channel_offset.reshape(1, -1),
        head_log_decay.T,
        context_step_logits.T,
        head_gate_rows.T,
        head_norm_scale.reshape(1, -1),
        residual,
        expert_norm_scale.reshape(1, -1),
        expert_index_table.T,
        expert_router_scores.T,
        mixer_output_weight,
        jnp.swapaxes(expert_gate_weight, 1, 2),
        jnp.swapaxes(expert_up_weight, 1, 2),
        expert_down_weight,
    )
    return total.astype(b16)


def solution(mesh):
    return jax.shard_map(
        shards,
        mesh=mesh,
        in_specs=(
            P("sp", "tp"),
            P("sp", "tp"),
            P("sp", "tp"),
            P("sp", "tp"),
            P("tp"),
            P("sp", "tp"),
            P("sp", "tp"),
            P("sp", "tp"),
            P("tp"),
            P(),
            P(("sp", "tp"), None),
            P(),
            P(("sp", "tp"), None),
            P(("sp", "tp"), None),
            P("sp", None, "tp"),
            P("sp", None, "tp"),
            P("sp", "tp", None),
        ),
        out_specs=P(("sp", "tp"), None),
        check_vma=False,
    )
```

```python
import jax
import jax.numpy as jnp
from jax import lax
from jax.experimental import pallas as pl
from jax.experimental.pallas import tpu as pltpu
from jax.sharding import PartitionSpec as P

HEAD_CHANNELS = 64

decay_factor = 0.6065306597126334
group_eps = 0.00064
norm_eps = 1e-06
key_eps = 1e-06
seq_len = 256
chunk_len = 32
chunks = seq_len // chunk_len


def split_two(value):
    top = value.astype(jnp.bfloat16)
    return top, (value - top.astype(jnp.float32)).astype(jnp.bfloat16)


def dot_f32(left, right, dims=(((1,), (0,)), ((), ()))):
    return lax.dot_general(left, right, dims, preferred_element_type=jnp.float32)


def product(left, right):
    left_top, left_low = split_two(left)
    right_top, right_low = split_two(right)
    return dot_f32(
        jnp.concatenate([left_top, left_top, left_low], axis=1),
        jnp.concatenate([right_top, right_low, right_top], axis=0),
    )


def product_nt(left, right):
    left_top, left_low = split_two(left)
    right_top, right_low = split_two(right)
    return dot_f32(
        jnp.concatenate([left_top, left_top, left_low], axis=1),
        jnp.concatenate([right_top, right_low, right_top], axis=1),
        (((1,), (1,)), ((), ())),
    )


def sigmoid(value):
    return 1.0 / (1.0 + jnp.exp(-value))


def turned(value):
    return jnp.transpose(value.astype(jnp.float32))


def mixer_local(receptance, key_matrix, value_t, decay_input, decay_offset, head_decay, step_logits):
    read_vec, key_vec = turned(receptance), turned(key_matrix)
    value_matrix = turned(value_t).astype(jnp.bfloat16)
    head_column = turned(jnp.broadcast_to(head_decay, (8, seq_len)))[:, 0:1]
    log_decay = head_column - decay_factor * sigmoid(turned(decay_input) + decay_offset)
    learn = turned(sigmoid(step_logits.astype(jnp.float32)))
    unit = key_vec * lax.rsqrt(jnp.sum(key_vec * key_vec, axis=1, keepdims=True) + key_eps)
    write = unit * learn
    keyed = key_vec * learn

    row = lax.broadcasted_iota(jnp.int32, (seq_len, seq_len), 0)
    col = lax.broadcasted_iota(jnp.int32, (seq_len, seq_len), 1)
    same = (row >> 5) == (col >> 5)
    upto = same & (col <= row)
    before = same & (col < row)

    log_top, log_rest = split_two(log_decay)
    log_low = (log_decay - log_top.astype(jnp.float32) - log_rest.astype(jnp.float32)).astype(jnp.bfloat16)
    summed = dot_f32(
        jnp.where(upto, 1.0, 0.0).astype(jnp.bfloat16),
        jnp.concatenate([log_top, log_rest, log_low], axis=1),
    )
    total = summed[:, :64] + summed[:, 64:128] + summed[:, 128:192]
    by_chunk = total.reshape(chunks, chunk_len, HEAD_CHANNELS)
    middle = jnp.broadcast_to(by_chunk[:, chunk_len // 2 - 1 : chunk_len // 2], by_chunk.shape).reshape(total.shape)
    last = by_chunk[:, chunk_len - 1 : chunk_len]
    ending = jnp.broadcast_to(last, by_chunk.shape).reshape(total.shape)
    prior = total - log_decay

    up_scale = jnp.exp(middle - total)
    scaled = jnp.concatenate([write * up_scale, keyed * up_scale], axis=0)
    gram = product_nt(-unit * jnp.exp(prior - middle), scaled)
    erase_write = jnp.where(before, gram[:, :seq_len], 0.0)
    erase_keyed = jnp.where(before, gram[:, seq_len:], 0.0)

    def below(width):
        return (
            ((row & (-2 * width)) == (col & (-2 * width)))
            & ((row & width) != 0)
            & ((col & width) == 0)
        )

    solved = jnp.where(row == col, 1.0, 0.0) + jnp.where(below(1), erase_write, 0.0)
    for width in (2, 4, 8, 16):
        solved = solved + product(solved, product(jnp.where(below(width), erase_write, 0.0), solved))

    def on_values(weights):
        top, low = split_two(weights)
        return dot_f32(
            jnp.concatenate([top, low], axis=1),
            jnp.concatenate([value_matrix, value_matrix], axis=0),
        )

    erased = product(
        solved, jnp.concatenate([-unit * jnp.exp(prior), on_values(erase_keyed)], axis=1)
    )
    tail_scale = jnp.exp(ending - total)
    wide_row = lax.broadcasted_iota(jnp.int32, (seq_len, chunks * 64), 0)
    wide_col = lax.broadcasted_iota(jnp.int32, (seq_len, chunks * 64), 1)
    in_block = (wide_row >> 5) == (wide_col >> 6)
    write_tail = jnp.where(in_block, jnp.concatenate([write * tail_scale] * chunks, axis=1), 0.0)
    keyed_tail = jnp.where(in_block, jnp.concatenate([keyed * tail_scale] * chunks, axis=1), 0.0)
    erased_t = jnp.transpose(erased)
    maps = product(erased_t, write_tail)
    keyed_top, keyed_low = split_two(keyed_tail)
    adds = maps[64:] + dot_f32(
        jnp.concatenate([value_t, value_t], axis=1),
        jnp.concatenate([keyed_top, keyed_low], axis=0),
    )
    small_row = lax.broadcasted_iota(jnp.int32, (64, 64), 0)
    small_col = lax.broadcasted_iota(jnp.int32, (64, 64), 1)
    eye = small_row == small_col

    def joined(early, late):
        moved = product(early, late[:64])
        return jnp.concatenate([moved[:64], moved[64:] + late[64:]], axis=0)

    steps = []
    for c in range(chunks):
        step_map = maps[:64, c * 64 : (c + 1) * 64] + jnp.where(eye, jnp.exp(last[c]), 0.0)
        steps.append(jnp.concatenate([step_map, adds[:, c * 64 : (c + 1) * 64]], axis=0))
    pairs = [joined(steps[2 * i], steps[2 * i + 1]) for i in range(4)]
    quads = [joined(pairs[0], pairs[1]), joined(pairs[2], pairs[3])]

    def outputs():
        gram_read = product_nt(read_vec * jnp.exp(total - middle), scaled)
        read_write = jnp.where(upto, gram_read[:, :seq_len], 0.0)
        read_keyed = jnp.where(upto, gram_read[:, seq_len:], 0.0)
        shown = product(read_write, erased)
        seen = read_vec * jnp.exp(total) + shown[:, :64]
        own = shown[:, 64:] + on_values(read_keyed)
        six = joined(quads[0], pairs[2])
        entering = (
            steps[0],
            pairs[0],
            joined(pairs[0], steps[2]),
            quads[0],
            joined(quads[0], steps[4]),
            six,
            joined(six, steps[6]),
        )
        through = [seen[:chunk_len]]
        local = [own[:chunk_len]]
        for c in range(1, chunks):
            part = slice(c * chunk_len, (c + 1) * chunk_len)
            viewed = product_nt(seen[part], entering[c - 1])
            through.append(viewed[:, :64])
            local.append(viewed[:, 64:] + own[part])
        return jnp.concatenate(through, axis=0), jnp.concatenate(local, axis=0)

    return joined(quads[0], quads[1]), outputs


MESH = pl.DeviceIdType.MESH
sub_rows = 16
subs = 4
half = 1024
width = 2048


def transfer(source, target, send, arrive, sp, tp):
    return pltpu.make_async_remote_copy(
        src_ref=source,
        dst_ref=target,
        send_sem=send,
        recv_sem=arrive,
        device_id=(sp, tp),
        device_id_type=MESH,
    )


def settle(block, sem):
    pltpu.make_async_copy(block, block, sem).wait()


def split_three(value):
    top, low = split_two(value)
    return top, low, (value - top.astype(jnp.float32) - low.astype(jnp.float32)).astype(jnp.bfloat16)


def ranks_of(first, second):
    count = first.shape[0]
    lane = lax.broadcasted_iota(jnp.int32, (count, 128), 1).astype(jnp.float32)
    hit_0 = jnp.where(lane == first, 1.0, 0.0)
    hit_1 = jnp.where(lane == second, 1.0, 0.0)
    row = lax.broadcasted_iota(jnp.int32, (count, count), 0)
    col = lax.broadcasted_iota(jnp.int32, (count, count), 1)
    same = (row >> 4) == (col >> 4)
    earlier = dot_f32(
        jnp.where(same & (col < row), 1.0, 0.0).astype(jnp.bfloat16),
        jnp.concatenate([hit_0, hit_1], axis=1).astype(jnp.bfloat16),
    )
    every = dot_f32(jnp.where(same, 1.0, 0.0).astype(jnp.bfloat16), hit_0.astype(jnp.bfloat16))
    rank_0 = jnp.sum(earlier[:, :128] * hit_0, axis=1, keepdims=True)
    rank_1 = jnp.sum((earlier[:, 128:] + every) * hit_1, axis=1, keepdims=True)
    return rank_0, rank_1


def fold_states(states):
    nodes = []
    for i in range(8):
        early, late = states[2 * i], states[2 * i + 1]
        stacked = jnp.concatenate([early[:, :64], early[:, 64:]], axis=0)
        moved = dot_f32(stacked, late[:, :64])
        nodes.append((moved[:64], moved[64:] + late[:, 64:].astype(jnp.float32)))
    while len(nodes) > 1:
        joined = []
        for i in range(0, len(nodes), 2):
            (early_map, early_state), (late_map, late_state) = nodes[i], nodes[i + 1]
            if i == 0:
                joined.append((None, product(early_state, late_map) + late_state))
            else:
                moved = product(jnp.concatenate([early_map, early_state], axis=0), late_map)
                joined.append((moved[:64], moved[64:] + late_state))
        nodes = joined
    return nodes[0][1]


def finish(mixer_out, head_norm_scale, head_gate_rows):
    average = jnp.mean(mixer_out, axis=1, keepdims=True)
    centred = mixer_out - average
    spread = jnp.mean(centred * centred, axis=1, keepdims=True)
    return centred * lax.rsqrt(spread + group_eps) * head_norm_scale * head_gate_rows


def layer_kernel(
    r_ref,
    k_ref,
    v_ref,
    d_ref,
    o_ref,
    h_ref,
    c_ref,
    g_ref,
    scale_ref,
    residual_ref,
    norm_ref,
    index_ref,
    score_ref,
    mix_hbm,
    gate_hbm,
    up_hbm,
    down_hbm,
    out_ref,
    mix_mat,
    gate_mat,
    up_mat,
    down_mat,
    gate_nat,
    up_nat,
    through_ref,
    local_ref,
    state_out,
    states,
    heads_out,
    heads_in,
    mixed_ref,
    table_ref,
    outgoing,
    incoming,
    raw_out,
    raw_in,
    far_out,
    far_in,
    codes,
    rows_all,
    gate_act,
    hidden_rows,
    mine_part,
    pair_out,
    pair_in,
    leave,
    back,
    sent_sum,
    pair_out_s,
    pair_in_s,
    leave_s,
    back_s,
    sent_sum_s,
    got_sum,
    weight_sem,
    state_send,
    state_recv,
    single_sem,
    spread_recv,
    ring_recv,
    twin_recv,
    pair_send,
    pair_recv,
    back_send,
    back_recv,
):
    sp, tp = lax.axis_index("sp"), lax.axis_index("tp")
    level, core = tp // 2, tp % 2
    twin = level * 2 + (1 - core)
    opposite = (tp + 8) % 16
    (
        heads_send,
        heads_recv,
        spread_send,
        ring_send,
        twin_send,
        sum_send,
        sum_recv,
        raw_send,
        raw_recv,
        far_send,
        far_recv,
    ) = (single_sem.at[k] for k in range(11))

    loads = [
        pltpu.make_async_copy(source, target, weight_sem.at[k])
        for k, (source, target) in enumerate(
            (
                (mix_hbm, mix_mat),
                (gate_hbm.at[0], gate_mat),
                (up_hbm.at[0], up_mat),
                (down_hbm.at[0], down_mat),
            )
        )
    ]
    for load in loads:
        load.start()

    start_row = lax.broadcasted_iota(jnp.int32, (16, 64, 128), 1)
    start_col = lax.broadcasted_iota(jnp.int32, (16, 64, 128), 2)
    states[...] = jnp.where(start_row == start_col, 1.0, 0.0).astype(jnp.bfloat16)

    barrier = pltpu.get_barrier_semaphore()
    for j in range(1, 16):
        pl.semaphore_signal(barrier, inc=1, device_id=((sp + j) % 16, tp), device_id_type=MESH)
        pl.semaphore_signal(barrier, inc=1, device_id=(sp, (tp + j) % 16), device_id_type=MESH)

    final, outputs = mixer_local(
        r_ref[...], k_ref[...], v_ref[...], d_ref[...], o_ref[...], h_ref[...], c_ref[...]
    )
    state_out[...] = jnp.concatenate([final[:64], final[64:]], axis=1).astype(jnp.bfloat16)
    own_table = jnp.transpose(
        jnp.concatenate(
            [
                jnp.concatenate([index_ref[...].astype(jnp.float32), score_ref[...]], axis=0),
                jnp.zeros((4, 112), jnp.float32),
            ],
            axis=1,
        )
    )[:16]
    table_ref[...] = own_table

    pl.semaphore_wait(barrier, 30)

    def state_copy(j, source, target):
        return transfer(
            state_out, states.at[source], state_send.at[j], state_recv.at[source], target, tp
        )

    for j in range(1, 16):

        @pl.when(sp + j < 16)
        def _():
            state_copy(j, sp, sp + j).start()

    through_ref[...], local_ref[...] = outputs()

    own_table = table_ref[...]
    rank_0, rank_1 = ranks_of(own_table[:, 0:1], own_table[:, 1:2])

    def spread_of(first, second):
        lane = lax.broadcasted_iota(jnp.int32, (16, 256), 1).astype(jnp.float32)
        return jnp.transpose(
            jnp.concatenate(
                [
                    jnp.where((lane == first + 4.0 * q) | (lane == second + 4.0 * q), 1.0, 0.0)
                    for q in range(4)
                ],
                axis=0,
            )
        ).astype(jnp.bfloat16)

    def spread_rows(spread, rows):
        stacked = jnp.concatenate([rows[:, q * 512 : (q + 1) * 512] for q in range(4)], axis=0)
        return dot_f32(spread, stacked).astype(jnp.bfloat16).reshape(16, 16, 512)

    spread = spread_of(own_table[:, 0:1] * 16.0 + rank_0, own_table[:, 1:2] * 16.0 + rank_1)

    for j in range(1, 16):

        @pl.when(sp - j >= 0)
        def _():
            state_copy(j, sp - j, sp).wait_recv()

    entering = fold_states(states[...])
    attended = finish(
        local_ref[...] + product_nt(through_ref[...], entering), scale_ref[...], turned(g_ref[...])
    )
    score_parts = [
        part for k in (2, 3) for part in split_three(own_table[:, k : k + 1])
    ]
    notes = jnp.concatenate(
        [own_table[:, 0:2].astype(jnp.bfloat16)] + score_parts + [jnp.zeros((16, 56), jnp.bfloat16)],
        axis=1,
    ).astype(jnp.float32)
    notes = jnp.broadcast_to(
        jnp.concatenate([notes, notes], axis=1)[None], (16, 16, 128)
    )
    both = jnp.concatenate([attended, attended], axis=1).reshape(16, 16, 128)
    side_lane = lax.broadcasted_iota(jnp.int32, (16, 16, 128), 2) // 64
    heads_out[...] = jnp.where(side_lane == core, both, notes).astype(jnp.bfloat16)
    for j in range(1, 16):
        other = (tp + j) % 16
        transfer(
            heads_out.at[other], heads_in.at[tp], heads_send, heads_recv, sp, other
        ).start()
    heads_in[tp] = heads_out[tp]

    for load in loads:
        load.wait()
    gate_nat[...] = jnp.transpose(gate_mat[...])

    settle(heads_in.at[pl.ds(0, 15)], heads_recv)
    low_lane = lax.broadcasted_iota(jnp.int32, (16, 128), 1) < 64
    tokens = jnp.concatenate(
        [
            jnp.where(
                low_lane,
                heads_in[2 * i].astype(jnp.float32),
                heads_in[2 * i + 1].astype(jnp.float32),
            ).astype(jnp.bfloat16)
            for i in range(8)
        ],
        axis=1,
    )
    mixed_f = (
        (residual_ref[...].astype(jnp.float32) + dot_f32(tokens, mix_mat[...]))
        .astype(jnp.bfloat16)
        .astype(jnp.float32)
    )
    mixed_ref[...] = mixed_f
    normed = (
        mixed_f
        * lax.rsqrt(jnp.mean(mixed_f * mixed_f, axis=1, keepdims=True) + norm_eps)
        * norm_ref[...]
    ).astype(jnp.bfloat16)
    raw_out[...] = normed
    raw_copy = transfer(raw_out, raw_in, raw_send, raw_recv, sp, opposite)
    raw_copy.start()
    outgoing[...] = spread_rows(spread, normed)
    row_at, col_at = sp // 4, sp % 4

    def spread_copy(source, target, at):
        return transfer(
            outgoing.at[target], incoming.at[source], spread_send, spread_recv.at[at], target, tp
        )

    for i in range(4):
        for k in range(4):
            if i == 0 and k == 0:
                continue
            other = ((row_at + 4 - i) % 4) * 4 + (col_at + k) % 4
            spread_copy(sp, other, i).start()
    incoming[sp] = outgoing[sp]

    noted = heads_in[...].astype(jnp.float32)
    every = jnp.concatenate(
        [noted[t][:, (1 - t % 2) * 64 : (1 - t % 2) * 64 + 8] for t in range(16)], axis=0
    )
    score_0 = every[:, 2:3] + every[:, 3:4] + every[:, 4:5]
    score_1 = every[:, 5:6] + every[:, 6:7] + every[:, 7:8]
    rank_0, rank_1 = ranks_of(every[:, 0:1], every[:, 1:2])
    gap = score_1 - score_0
    wide_lane = lax.broadcasted_iota(jnp.int32, (256, 128), 1)
    kept = jnp.zeros((256, 128), jnp.float32)
    for at, column in enumerate(
        (
            every[:, 0:1] * 16.0 + rank_0,
            every[:, 1:2] * 16.0 + rank_1,
            1.0 / (1.0 + jnp.exp(gap)),
            1.0 / (1.0 + jnp.exp(-gap)),
            every[:, 0:1] * 8.0 + rank_0,
            every[:, 1:2] * 8.0 + rank_1,
        )
    ):
        kept = jnp.where(wide_lane == at, column, kept)
    codes[...] = kept.reshape(16, 16, 128)
    up_nat[...] = jnp.transpose(up_mat[...])

    following = (((level + 1) % 8) * 2 + core, ((level + 7) % 8) * 2 + core)

    def block_at(distance, way):
        if way == 0:
            return (level + 8 - distance) % 8
        return (level + distance) % 8

    def turn(sub):
        return (row_at + sub) % 4

    def piece_of(index, sub):
        return rows_all.at[index, pl.ds(pl.multiple_of(turn(sub) * sub_rows, sub_rows), sub_rows)]

    def arrival(distance, sub):
        return (distance - 1) * subs + sub

    def ring(index, sub, distance, way):
        slot = arrival(distance, sub)
        return transfer(
            piece_of(index, sub),
            piece_of(index, sub),
            ring_send,
            ring_recv.at[way, slot],
            sp,
            following[way],
        )

    def twinned(index, sub, piece):
        return transfer(
            piece_of(index, sub), piece_of(index, sub), twin_send, twin_recv.at[piece], sp, twin
        )

    small_row = lax.broadcasted_iota(jnp.int32, (64, 64), 0)
    small_col = lax.broadcasted_iota(jnp.int32, (64, 64), 1)
    regroup = jnp.where(
        small_col == ((small_row >> 2) & 3) * 16 + (small_row >> 4) * 4 + (small_row & 3), 1.0, 0.0
    ).astype(jnp.bfloat16)
    for sub in range(subs):
        settle(incoming.at[pl.ds(0, 3 if sub == 0 else 4)], spread_recv.at[sub])
        regrouped = dot_f32(
            regroup, incoming[pl.ds(turn(sub) * 4, 4)].reshape(64, 512)
        ).astype(jnp.bfloat16)
        rows_all[tp, pl.ds(pl.multiple_of(turn(sub) * sub_rows, sub_rows), sub_rows)] = (
            jnp.concatenate([regrouped[q * 16 : (q + 1) * 16] for q in range(4)], axis=1)
        )
        for way in (0, 1):
            ring(tp, sub, 1, way).start()
        twinned(tp, sub, 0).start()

    raw_copy.wait_recv()
    far_codes = codes[opposite]
    far_out[...] = spread_rows(spread_of(far_codes[:, 0:1], far_codes[:, 1:2]), raw_in[...])
    for j in range(1, 16):
        other = (sp + j) % 16
        transfer(far_out.at[other], far_in.at[sp], far_send, far_recv, other, tp).start()
    far_in[sp] = far_out[sp]

    def far_arrives():
        settle(far_in.at[pl.ds(0, 15)], far_recv)
        for sub in range(subs):
            regrouped = dot_f32(
                regroup, far_in[sub * 4 : (sub + 1) * 4].reshape(64, 512)
            ).astype(jnp.bfloat16)
            rows_all[opposite, sub * sub_rows : (sub + 1) * sub_rows] = jnp.concatenate(
                [regrouped[q * 16 : (q + 1) * 16] for q in range(4)], axis=1
            )
        transfer(
            rows_all.at[opposite], rows_all.at[opposite], twin_send, twin_recv.at[4], sp, twin
        ).start()

    def forward(distance, sub):
        for way in (0, 1):
            index = block_at(distance, way) * 2 + core
            ring(index, sub, distance, way).wait_recv()
            if distance < 3:
                ring(index, sub, distance + 1, way).start()
            piece = distance
            if distance == 3 and way == 1:
                piece = 5
            if distance == 1 and sub > 1:
                piece = 6
            twinned(index, sub, piece).start()

    def await_twin(distance):
        settle(rows_all.at[pl.ds(0, 2 if distance == 2 else 1)], twin_recv.at[distance])

    def members(distance):
        if distance == 6:
            distance = 1
        low = block_at(3, 1) * 2 if distance == 5 else block_at(distance, 0) * 2
        if distance not in (1, 2, 6):
            return (low, low + 1)
        high = block_at(distance, 1) * 2
        return (low, low + 1, high, high + 1)

    def buffers(distance):
        if distance not in (1, 2, 6):
            at = (0, None, None, 2, 1, 3)[distance]
            return (
                pair_out_s.at[at],
                pair_in_s.at[at],
                leave_s.at[at],
                back_s.at[at],
                sent_sum_s.at[at],
            )
        at = 1 if distance == 2 else 0
        return pair_out.at[at], pair_in.at[at], leave.at[at], back.at[at], sent_sum.at[at]

    def order_of(parts):
        count = parts * 64
        row = lax.broadcasted_iota(jnp.int32, (count, count), 0)
        col = lax.broadcasted_iota(jnp.int32, (count, count), 1)
        source = ((row >> 2) & (parts - 1)) * 64 + (row // (4 * parts)) * 4 + (row & 3)
        return jnp.where(col == source, 1.0, 0.0).astype(jnp.bfloat16)

    reorder = {2: order_of(2), 4: order_of(4)}
    half_row = lax.broadcasted_iota(jnp.int32, (128, 128), 0)
    half_col = lax.broadcasted_iota(jnp.int32, (128, 128), 1)
    half_order = jnp.where(
        half_col == ((half_row >> 2) & 3) * 32 + (half_row >> 4) * 4 + (half_row & 3), 1.0, 0.0
    ).astype(jnp.bfloat16)

    def part_of(distance):
        return pl.ds(128 if distance == 6 else 0, 256 if distance == 2 else 128)
    core_at = pl.multiple_of(core * half, half)
    twin_at = pl.multiple_of((1 - core) * half, half)
    across = (((1,), (1,)), ((), ()))

    def rows_in(distance):
        if distance in (1, 6):
            first = 0 if distance == 1 else 2
            return jnp.concatenate(
                [
                    piece_of(index, first + i)[...]
                    for index in members(distance)
                    for i in range(2)
                ],
                axis=0,
            )
        return jnp.concatenate([rows_all[index] for index in members(distance)], axis=0)

    def count_of(distance):
        return 256 if distance == 2 else 128

    def stage_gate(distance):
        count = count_of(distance)
        gate_act[:count] = dot_f32(rows_in(distance), gate_nat[...])

    def stage_up(distance):
        count = count_of(distance)
        order = half_order if distance in (1, 6) else reorder[count // 64]
        up_act = dot_f32(rows_in(distance), up_nat[...])
        gate = gate_act[:count]
        hidden = (gate / (1.0 + jnp.exp(-gate)) * up_act).astype(jnp.bfloat16)
        hidden_rows[:count] = dot_f32(order, hidden).astype(jnp.bfloat16)

    def pair(distance):
        out, arrived = buffers(distance)[:2]
        out, arrived = out.at[part_of(distance)], arrived.at[part_of(distance)]
        return transfer(out, arrived, pair_send.at[distance], pair_recv.at[distance], sp, twin)

    def stage_other(distance):
        count = count_of(distance)
        buffers(distance)[0][part_of(distance)] = dot_f32(
            hidden_rows[:count], down_mat[:, pl.ds(twin_at, half)]
        ).astype(jnp.bfloat16)
        pair(distance).start()

    def stage_mine(distance):
        count = count_of(distance)
        mine_part[:count] = dot_f32(hidden_rows[:count], down_mat[:, pl.ds(core_at, half)])

    def back_copy(distance, source, target):
        _, _, out, arrived, _ = buffers(distance)
        return transfer(
            out.at[target],
            arrived.at[source],
            back_send.at[1 if distance == 6 else distance],
            back_recv.at[1 if distance == 6 else distance],
            target,
            tp,
        )

    def stage_return(distance):
        parts = len(members(distance))
        _, arrived, out, home, _ = buffers(distance)
        pair(distance).wait_recv()
        if distance in (1, 6):
            summed = (
                (mine_part[:128] + arrived[part_of(distance)].astype(jnp.float32))
                .astype(jnp.bfloat16)
                .reshape(8, 16, half)
            )
            for i in range(2):
                sub = i + (0 if distance == 1 else 2)
                out[pl.ds(turn(sub) * 4, 4)] = summed[i * 4 : (i + 1) * 4]
            for i in range(2):
                sub = i + (0 if distance == 1 else 2)
                for k in range(4):
                    if sub == 0 and k == 0:
                        continue
                    back_copy(distance, sp, turn(sub) * 4 + (col_at + k) % 4).start()
            if distance == 1:
                home[sp] = out[sp]
            return
        out[...] = (
            (mine_part[: 64 * parts] + arrived[...].astype(jnp.float32))
            .reshape(16, 4 * parts, half)
            .astype(jnp.bfloat16)
        )
        for j in range(1, 16):
            back_copy(distance, sp, (sp + j) % 16).start()
        home[sp] = out[sp]

    def stage_combine(distance):
        parts = len(members(distance))
        _, _, _, home, leaving = buffers(distance)
        settle(home.at[pl.ds(0, 15)], back_recv.at[distance])
        column = 0 if parts == 4 else 4
        columns = 64 * parts
        lanes = lax.broadcasted_iota(jnp.int32, (16, columns), 1).astype(jnp.float32)
        weights = []
        for place_in, index in enumerate(members(distance)):
            code = codes[index]
            first_at = code[:, column : column + 1] + 4.0 * place_in
            second_at = code[:, column + 1 : column + 2] + 4.0 * place_in
            weights.append(
                jnp.where(lanes == first_at, code[:, 2:3], 0.0)
                + jnp.where(lanes == second_at, code[:, 3:4], 0.0)
            )
        top, low = split_two(jnp.concatenate(weights, axis=0))
        returned = (
            home[...].astype(jnp.float32).reshape(columns, half).astype(jnp.bfloat16)
            if parts == 2
            else home[...].reshape(columns, half)
        )
        leaving[...] = (
            (dot_f32(top, returned) + dot_f32(low, returned)).astype(jnp.bfloat16).reshape(parts, 16, half)
        )

        def send(place_in, index):
            transfer(leaving.at[place_in], got_sum.at[tp], sum_send, sum_recv, sp, index).start()

        if distance == 0:
            send(1 - core, twin)
            got_sum[tp] = leaving[core]
        else:
            for place_in, index in enumerate(members(distance)):
                send(place_in, index)

    def stages_up(distance):
        await_twin(distance)
        stage_gate(distance)
        stage_up(distance)

    def stages_down(distance):
        stage_other(distance)
        stage_mine(distance)

    stages_up(0)
    forward(1, 0)
    stages_down(0)
    forward(1, 1)
    stage_return(0)
    stages_up(1)
    forward(1, 2)
    stages_down(1)
    forward(1, 3)
    stage_return(1)
    stages_up(6)
    forward(2, 0)
    stages_down(6)
    far_arrives()
    forward(2, 1)
    stage_return(6)
    forward(2, 2)
    stages_up(4)
    stages_down(4)
    forward(2, 3)
    stage_return(4)
    stages_up(2)
    forward(3, 0)
    stages_down(2)
    forward(3, 1)
    stage_return(2)
    forward(3, 2)
    stage_combine(0)
    forward(3, 3)
    stages_up(3)
    stages_down(3)
    stage_combine(1)
    stages_up(5)
    stage_return(3)
    stages_down(5)
    stage_combine(4)
    stage_return(5)
    stage_combine(2)
    stage_combine(3)
    stage_combine(5)

    settle(got_sum.at[pl.ds(0, 15)], sum_recv)
    for side in (0, 1):
        gathered = got_sum[side].astype(jnp.float32)
        for stage in range(1, 8):
            gathered = gathered + got_sum[2 * stage + side].astype(jnp.float32)
        cut = slice(side * half, (side + 1) * half)
        out_ref[:, cut] = mixed_ref[:, cut] + gathered
    settle(heads_out.at[pl.ds(0, 15)], heads_send)
    settle(outgoing.at[pl.ds(0, 15)], spread_send)
    settle(rows_all.at[pl.ds(0, 6)], ring_send)
    settle(raw_out, raw_send)
    settle(far_out.at[pl.ds(0, 15)], far_send)
    settle(rows_all.at[pl.ds(0, 8)], twin_send)
    settle(got_sum.at[pl.ds(0, 15)], sum_send)
    pair(6).wait_send()
    for distance in range(6):
        pair(distance).wait_send()
        settle(buffers(distance)[2].at[pl.ds(0, 15)], back_send.at[distance])
    for j in range(1, 16):

        @pl.when(sp + j < 16)
        def _():
            state_copy(j, sp, sp + j).wait_send()


def shards(
    receptance,
    key_matrix,
    value_matrix,
    decay_input_term,
    decay_channel_offset,
    head_log_decay,
    context_step_logits,
    head_gate_rows,
    head_norm_scale,
    mixer_output_weight,
    residual,
    expert_norm_scale,
    expert_index_table,
    expert_router_scores,
    expert_gate_weight,
    expert_up_weight,
    expert_down_weight,
):
    vmem = pl.BlockSpec(memory_space=pltpu.VMEM)
    hbm = pl.BlockSpec(memory_space=pl.ANY)
    dma = pltpu.SemaphoreType.DMA
    b16, f32 = jnp.bfloat16, jnp.float32
    total = pl.pallas_call(
        layer_kernel,
        out_shape=jax.ShapeDtypeStruct((16, width), f32),
        in_specs=[vmem] * 13 + [hbm] * 4,
        out_specs=vmem,
        scratch_shapes=[
            pltpu.VMEM((1024, width), b16),
            pltpu.VMEM((448, width), b16),
            pltpu.VMEM((448, width), b16),
            pltpu.VMEM((448, width), b16),
            pltpu.VMEM((width, 448), b16),
            pltpu.VMEM((width, 448), b16),
            pltpu.VMEM((seq_len, 64), f32),
            pltpu.VMEM((seq_len, 64), f32),
            pltpu.VMEM((64, 128), b16),
            pltpu.VMEM((16, 64, 128), b16),
            pltpu.VMEM((16, 16, 128), b16),
            pltpu.VMEM((16, 16, 128), b16),
            pltpu.VMEM((16, width), f32),
            pltpu.VMEM((16, 4), f32),
            pltpu.VMEM((16, 16, 512), b16),
            pltpu.VMEM((16, 16, 512), b16),
            pltpu.VMEM((16, width), b16),
            pltpu.VMEM((16, width), b16),
            pltpu.VMEM((16, 16, 512), b16),
            pltpu.VMEM((16, 16, 512), b16),
            pltpu.VMEM((16, 16, 128), f32),
            pltpu.VMEM((16, 64, width), b16),
            pltpu.VMEM((256, 448), f32),
            pltpu.VMEM((256, 448), b16),
            pltpu.VMEM((256, half), f32),
            pltpu.VMEM((2, 256, half), b16),
            pltpu.VMEM((2, 256, half), b16),
            pltpu.VMEM((2, 16, 16, half), b16),
            pltpu.VMEM((2, 16, 16, half), b16),
            pltpu.VMEM((2, 4, 16, half), b16),
            pltpu.VMEM((4, 128, half), b16),
            pltpu.VMEM((4, 128, half), b16),
            pltpu.VMEM((4, 16, 8, half), b16),
            pltpu.VMEM((4, 16, 8, half), b16),
            pltpu.VMEM((4, 2, 16, half), b16),
            pltpu.VMEM((16, 16, half), b16),
            dma((4,)),
            dma((16,)),
            dma((16,)),
            dma((11,)),
            dma((4,)),
            dma((2, 12)),
        ]
        + [dma((7,))] * 5,
        compiler_params=pltpu.CompilerParams(
            collective_id=1, has_side_effects=True, vmem_limit_bytes=56 * 1024 * 1024
        ),
    )(
        receptance.T,
        key_matrix.T,
        value_matrix.T,
        decay_input_term.T,
        decay_channel_offset.reshape(1, -1),
        head_log_decay.T,
        context_step_logits.T,
        head_gate_rows.T,
        head_norm_scale.reshape(1, -1),
        residual,
        expert_norm_scale.reshape(1, -1),
        expert_index_table.T,
        expert_router_scores.T,
        mixer_output_weight,
        jnp.swapaxes(expert_gate_weight, 1, 2),
        jnp.swapaxes(expert_up_weight, 1, 2),
        expert_down_weight,
    )
    return total.astype(b16)


def solution(mesh):
    return jax.shard_map(
        shards,
        mesh=mesh,
        in_specs=(
            P("sp", "tp"),
            P("sp", "tp"),
            P("sp", "tp"),
            P("sp", "tp"),
            P("tp"),
            P("sp", "tp"),
            P("sp", "tp"),
            P("sp", "tp"),
            P("tp"),
            P(),
            P(("sp", "tp"), None),
            P(),
            P(("sp", "tp"), None),
            P(("sp", "tp"), None),
            P("sp", None, "tp"),
            P("sp", None, "tp"),
            P("sp", "tp", None),
        ),
        out_specs=P(("sp", "tp"), None),
        check_vma=False,
    )
```
